32 devices in a mesh: rep: 2 (over x), fs: 8 (over z, y), tp: 2 (over core).
Axes of the slice: x: 2, y: 2, z: 4, core: 2. Of those that a mesh axis runs over, the one named last changes fastest.
Arguments:
- tokens: bfloat16 [256, 16, 2048], P('tp', ('rep', 'fs')), may hold values from -6 to 6
- mix_gain: float32 [2048], replicated, may hold values from 0.1 to 1.9
- value_weight: bfloat16 [2048, 1024], P('fs', 'tp'), may hold values from -0.125 to 0.125
- gate_weight: bfloat16 [2048, 1024], P('fs', 'tp'), may hold values from -0.125 to 0.125
- conv_taps: float32 [31, 1024], P(None, 'tp'), may hold values from -1 to 1
- head_gain: float32 [1024], P('tp'), may hold values from 0.1 to 1.9
- out_weight: bfloat16 [1024, 2048], P('tp', 'fs'), may hold values from -0.1875 to 0.1875
- ffn_gain: float32 [2048], replicated, may hold values from 0.1 to 1.9
- ffn_gate_weight: bfloat16 [2048, 3072], P('fs', 'tp'), may hold values from -0.125 to 0.125
- ffn_up_weight: bfloat16 [2048, 3072], P('fs', 'tp'), may hold values from -0.125 to 0.125
- down_weight: bfloat16 [3072, 2048], P('tp', 'fs'), may hold values from -0.109375 to 0.109375
Outputs:
- layer_out: bfloat16 [256, 16, 2048], P('tp', ('rep', 'fs'))
The draws below stay inside these ranges and needn't reach their ends.
All inputs are finite; a program needn't handle non-finite values.
Results may differ from the reference program's by a relative error of at most 0.012.
Values may be sent and summed in bfloat16 or wider, within the bound.
A program may use at most 128 MiB of HBM per device.

```python
import jax
import jax.numpy as jnp
from jax import lax

D = 2048
HEADS = 8
HEAD_DIM = 128
FF = 3072
KW = 31
LEN = 256
SEQ_DEV = 1
CH = 1024
BATCH = 16
N_TP = 2


def block_levels(stream_key, dims, pieces, low, high):
    loudness = 1.0
    for axis_at, parts in pieces:
        heights = jax.random.uniform(jax.random.fold_in(jax.random.fold_in(stream_key, 6), axis_at), (parts,), jnp.float32, low / len(pieces), high / len(pieces))
        loudness = loudness * jnp.repeat(jnp.exp(heights), dims[axis_at] // parts).reshape((-1,) + (1,) * (len(dims) - 1 - axis_at))
    return loudness


def centred(stream_key, extent, deviation, bound, shards=(), kind=jnp.bfloat16):
    gain = block_levels(stream_key, extent, shards, -0.22, 0.18) if shards else 1.0
    drawn = jax.random.normal(stream_key, extent, jnp.float32) * deviation * gain
    return jnp.minimum(jnp.maximum(drawn, -bound), bound).astype(kind)


def setup_inputs(seed: int = 0) -> dict:
    keys = jax.random.split(jax.random.key(seed), 12)
    return {
        "tokens": centred(keys[0], (LEN, BATCH, D), 1.0, 6.0, ((0, 2), (1, 16))),
        "mix_gain": jnp.clip(1.0 + 0.18 * jax.random.normal(keys[1], (D,), jnp.float32), 0.1, 1.9),
        "value_weight": centred(keys[2], (D, CH), D ** -0.5, 0.125, ((0, 8), (1, 2))),
        "gate_weight": centred(keys[3], (D, CH), D ** -0.5, 0.125, ((0, 8), (1, 2))),
        "conv_taps": centred(keys[4], (KW, CH), KW ** -0.5, 1.0, ((1, 2),), jnp.float32),
        "head_gain": jnp.clip(1.0 + 0.18 * jax.random.normal(keys[5], (CH,), jnp.float32), 0.1, 1.9),
        "out_weight": centred(keys[6], (CH, D), CH ** -0.5, 0.1875, ((0, 2), (1, 8))),
        "ffn_gain": jnp.clip(1.0 + 0.18 * jax.random.normal(keys[7], (D,), jnp.float32), 0.1, 1.9),
        "ffn_gate_weight": centred(keys[8], (D, FF), D ** -0.5, 0.125, ((0, 8), (1, 2))),
        "ffn_up_weight": centred(keys[9], (D, FF), D ** -0.5, 0.125, ((0, 8), (1, 2))),
        "down_weight": centred(keys[10], (FF, D), FF ** -0.5, 0.109375, ((0, 2), (1, 8))),
    }


norm_eps = 1e-06
group_eps = 1e-05

def rms_scale(matrix, scales):
    return matrix * lax.rsqrt(lax.optimization_barrier(jnp.mean(matrix * matrix, axis=-1, keepdims=True)) + norm_eps) * scales

def split_sum(activated, weights, block_width):
    summed = jnp.zeros((activated.shape[0], weights.shape[1]), jnp.float32)
    for block_idx in range(N_TP):
        lower = block_idx * block_width
        partial_value = jnp.dot(activated[:, lower:lower + block_width], weights[lower:lower + block_width], preferred_element_type=jnp.float32).astype(jnp.bfloat16)
        partial_value = lax.optimization_barrier(partial_value)
        summed = summed + partial_value.astype(jnp.float32)
    return summed

def reference(tokens, mix_gain, value_weight, gate_weight, conv_taps, head_gain, out_weight, ffn_gain, ffn_gate_weight, ffn_up_weight, down_weight):

    def sequence_block(inputs):
        seq_count = inputs.shape[1]
        residual = inputs.reshape(-1, D).astype(jnp.float32)
        normed = rms_scale(residual, mix_gain).astype(jnp.bfloat16)
        value_rows = jnp.dot(normed, value_weight, preferred_element_type=jnp.float32)
        gate_rows = jnp.dot(normed, gate_weight, preferred_element_type=jnp.float32)
        glu_rows = (value_rows * jax.nn.sigmoid(gate_rows)).astype(jnp.bfloat16).reshape(LEN, seq_count, CH)
        conved = lax.conv_general_dilated(glu_rows.astype(jnp.float32), conv_taps[:, None, :], (1,), [(KW // 2, KW // 2)], dimension_numbers=('WNC', 'WIO', 'WNC'), feature_group_count=CH, precision=lax.Precision.HIGHEST)
        grouped = conved.reshape(LEN, seq_count, HEADS, HEAD_DIM)
        head_mean = lax.optimization_barrier(jnp.mean(grouped, axis=-1, keepdims=True))
        head_var = lax.optimization_barrier(jnp.mean(jnp.square(grouped - head_mean), axis=-1, keepdims=True))
        scaled = (grouped - head_mean) * lax.rsqrt(head_var + group_eps) * head_gain.reshape(HEADS, HEAD_DIM)
        activated = jax.nn.silu(scaled).astype(jnp.bfloat16).reshape(-1, CH)
        mixed_rows = split_sum(activated, out_weight, CH // N_TP)
        middle = (residual + mixed_rows).astype(jnp.bfloat16)
        middle_f = middle.astype(jnp.float32)
        normed_ffn = rms_scale(middle_f, ffn_gain).astype(jnp.bfloat16)
        gate_part = jnp.dot(normed_ffn, ffn_gate_weight, preferred_element_type=jnp.float32)
        up_part = jnp.dot(normed_ffn, ffn_up_weight, preferred_element_type=jnp.float32)
        hidden = (jax.nn.silu(gate_part) * up_part).astype(jnp.bfloat16)
        fed_rows = split_sum(hidden, down_weight, FF // N_TP)
        return (middle_f + fed_rows).astype(jnp.bfloat16).reshape(inputs.shape)
    blocks = tokens.reshape(LEN, BATCH // SEQ_DEV, SEQ_DEV, D).transpose(1, 0, 2, 3)
    results = lax.map(sequence_block, blocks)
    return results.transpose(1, 0, 2, 3).reshape(LEN, BATCH, D)
```

```python
import functools

import jax
import jax.numpy as jnp
from jax import lax
from jax.experimental import pallas as pl
from jax.experimental.pallas import tpu as pltpu
from jax.sharding import PartitionSpec as P

HEAD_DIM = 128
MESH = pl.DeviceIdType.MESH

norm_eps = 1e-06
group_eps = 1e-05
f32 = jnp.float32
bf16 = jnp.bfloat16


def rms_scale(matrix, scales):
    return matrix * lax.rsqrt(jnp.mean(matrix * matrix, axis=-1, keepdims=True) + norm_eps) * scales


class Moves:
    def __init__(self, n_rep, n_fs, sources, wholes, offsets, axes, sems):
        self.rep, self.fs, self.tp = lax.axis_index("rep"), lax.axis_index("fs"), lax.axis_index("tp")
        rep, fs, tp = self.rep, self.fs, self.tp
        self.ring = n_fs // 2
        self.pair, self.place = fs % 2, fs // 2
        flip = fs + 1 - 2 * self.pair
        self.to_tp = (rep, fs, 1 - tp)
        self.peers = (None, (rep, flip, tp), (1 - rep, fs, tp), (1 - rep, flip, tp))
        self.after = (rep, (fs + 2) % n_fs, tp)
        self.before = (rep, (fs + n_fs - 2) % n_fs, tp)
        self.quarter = rep * 2 + self.pair
        self.other = rep * 2 + 1 - self.pair
        self.sources, self.wholes, self.offsets, self.axes = sources, wholes, offsets, axes
        self.ring_send, self.ring_recv, self.pair_send, self.pair_recv = sems

    def greet(self):
        for device in self.peers[1:] + (self.to_tp, self.after, self.before):
            pl.semaphore_signal(pltpu.get_barrier_semaphore(), inc=1, device_id=device, device_id_type=MESH)

    def meet(self):
        pl.semaphore_wait(pltpu.get_barrier_semaphore(), 6)

    def part(self, w, quarter):
        size = self.sources[w].shape[self.axes[w]] // 4
        at = pl.ds(pl.multiple_of(quarter * size, size), size)
        return (slice(None), at) if self.axes[w] == 1 else (at, slice(None))

    def slot(self, w, owner):
        if self.axes[w] == 0:
            return (owner,)
        size, columns = self.sources[w].shape
        at = pl.ds(pl.multiple_of(owner * size, size), size)
        return (at, pl.ds(self.offsets[w], columns // 4))

    def pair_copy(self, w):
        return pltpu.make_async_remote_copy(
            src_ref=self.sources[w].at[self.part(w, self.other)],
            dst_ref=self.wholes[w].at[self.slot(w, self.fs)],
            send_sem=self.pair_send.at[w],
            recv_sem=self.pair_recv.at[w],
            device_id=self.peers[1],
            device_id_type=MESH,
        )

    def ring_copy(self, w, p, s):
        parity = self.pair if p == 0 else 1 - self.pair
        owner = ((self.place + self.ring + 1 - s) % self.ring) * 2 + parity
        there = self.wholes[w].at[self.slot(w, owner)]
        here = self.sources[w].at[self.part(w, self.quarter)] if s == 1 and p == 0 else there
        return pltpu.make_async_remote_copy(
            src_ref=here,
            dst_ref=there,
            send_sem=self.ring_send.at[w, p, s - 1],
            recv_sem=self.ring_recv.at[w, p, s - 1],
            device_id=self.after,
            device_id_type=MESH,
        )

    def push(self, w, p, s):
        if s > 1:
            self.ring_copy(w, p, s - 1).wait_recv()
        elif p == 1:
            self.pair_copy(w).wait_recv()
        self.ring_copy(w, p, s).start()

    def arrived(self, w):
        for p in (0, 1):
            self.ring_copy(w, p, self.ring - 1).wait_recv()

    def sent(self):
        for w in range(len(self.sources)):
            self.pair_copy(w).wait_send()
            for p in (0, 1):
                for s in range(1, self.ring):
                    self.ring_copy(w, p, s).wait_send()

    def copy(self, src, dst, device, sems, i):
        return pltpu.make_async_remote_copy(
            src_ref=src,
            dst_ref=dst,
            send_sem=sems[0].at[i],
            recv_sem=sems[1].at[i],
            device_id=device,
            device_id_type=MESH,
        )


class RowGather:
    def __init__(self, m, own, rows, sems):
        half = own.shape[0] // 2
        low, high = pl.ds(0, half), pl.ds(half, half)
        _, pair, rep, _ = m.peers
        first, near_pair, near_rep, across = (2 * k + m.tp for k in range(4))
        moves = (
            (own.at[low], rows.at[near_rep, low], rep),
            (own.at[high], rows.at[near_pair, high], pair),
            (own.at[high], rows.at[near_rep, high], rep),
            (own.at[low], rows.at[near_pair, low], pair),
            (rows.at[near_rep, low], rows.at[across, low], pair),
            (rows.at[near_pair, high], rows.at[across, high], rep),
            (own, rows.at[first], m.to_tp),
            (rows.at[near_rep], rows.at[near_rep], m.to_tp),
            (rows.at[near_pair], rows.at[near_pair], m.to_tp),
            (rows.at[across, low], rows.at[across, low], m.to_tp),
            (rows.at[across, high], rows.at[across, high], m.to_tp),
        )
        self.copies = [m.copy(*move, sems, i) for i, move in enumerate(moves)]

    def start(self):
        for i in (0, 1, 2, 3, 6):
            self.copies[i].start()

    def forward(self):
        for i in (0, 1):
            self.copies[i].wait_recv()
            self.copies[i + 4].start()

    def finish(self):
        for i in (2, 3, 4, 5):
            self.copies[i].wait_recv()
            self.copies[i + 5].start()

    def ready(self, k):
        for i in ((6,), (8,), (7,), (9, 10))[k]:
            self.copies[i].wait_recv()

    def sent(self):
        for copy in self.copies:
            copy.wait_send()


VALUE, GATE, OUT, FFN_GATE, FFN_UP, DOWN = range(6)
AXES = (1, 1, 0, 1, 1, 0)


def layer_kernel(
    n_rep, n_fs, tokens_in, mix_gain_in, value, gate, taps_in, head_gain_in, out, ffn_gain_in, ffn_gate, ffn_up,
    down, result,
    *scratch,
):
    staged, scratch = scratch[:6], scratch[6:]
    module_q, out_q, ffn_q, down_q = scratch[:4]
    tokens, mix_gain, taps, head_gain, ffn_gain = scratch[4:9]
    rows_a, rows, padded, activated, hidden, middle, total, tp_out, tp_in, x_out, x_in, finished = scratch[9:21]
    ring_sems, scratch = scratch[21:25], scratch[25:]
    row_a_sems, row_sems, (sum_send, sum_recv), local_sem = scratch[:2], scratch[2:4], scratch[4:6], scratch[6]
    shards = (value, gate, out, ffn_gate, ffn_up, down)
    channels, units = out_q.shape[1], down_q.shape[1]
    wholes = (module_q, module_q, out_q, ffn_q, ffn_q, down_q)
    m = Moves(n_rep, n_fs, staged, wholes, (0, channels, None, 0, units, None), AXES, ring_sems)
    length, width = tokens.shape
    kernel = taps.shape[0]
    pad = (padded.shape[1] - 2 * length) // 2
    tile = 512
    high = 32
    near_at = pl.ds(pl.multiple_of(m.tp * length, length), length)
    far_at = pl.ds(pl.multiple_of((1 - m.tp) * length, length), length)

    local = [pltpu.make_async_copy(s, d, local_sem.at[i]) for i, (s, d) in enumerate(zip(shards, staged))]
    smalls = ((tokens_in, tokens), (mix_gain_in, mix_gain), (taps_in, taps))
    smalls += ((head_gain_in, head_gain), (ffn_gain_in, ffn_gain))
    small = [pltpu.make_async_copy(s, d, local_sem.at[6 + i]) for i, (s, d) in enumerate(smalls)]
    placed = []
    for w in range(6):
        placed.append(
            pltpu.make_async_copy(shards[w].at[m.part(w, m.quarter)], wholes[w].at[m.slot(w, m.fs)], local_sem.at[11 + w])
        )
    m.greet()
    for copy in local[:3] + small[:2] + placed[:2] + small[2:4] + placed[2:3] + local[3:] + placed[3:] + small[4:]:
        copy.start()
    for w in (VALUE, GATE, OUT):
        local[w].wait()
    m.meet()
    for w in (VALUE, GATE, OUT):
        m.pair_copy(w).start()
    for w in (VALUE, GATE, OUT):
        m.push(w, 0, 1)

    def module_norm(i, _):
        at = pl.ds(pl.multiple_of(i * high, high), high)
        rows_a[m.tp, at, :] = rms_scale(tokens[at, :].astype(f32), mix_gain[...]).astype(bf16)
        return _

    small[0].wait()
    small[1].wait()
    lax.fori_loop(0, length // high, module_norm, 0)
    gather = RowGather(m, rows_a.at[m.tp], rows_a, row_a_sems)
    gather.start()
    for w in (VALUE, GATE, OUT):
        m.push(w, 1, 1)
    for w in (FFN_GATE, FFN_UP, DOWN):
        local[w].wait()
    zeros = jnp.zeros((4, pad, channels), f32)
    padded[:, pl.ds(0, pad), :] = zeros
    padded[:, pl.ds(pad + 2 * length, pad), :] = zeros
    for s in range(2, m.ring):
        for p in (0, 1):
            for w in (VALUE, GATE, OUT):
                m.push(w, p, s)
        if s == 2:
            gather.forward()
    for w in (FFN_GATE, FFN_UP):
        m.pair_copy(w).start()
    for w in (FFN_GATE, FFN_UP):
        m.push(w, 0, 1)
    gather.finish()
    for copy in placed + small[2:]:
        copy.wait()
    m.arrived(VALUE)
    m.arrived(GATE)

    def gated(k):
        block = rows_a[pl.ds(2 * k, 2)].reshape(2 * length, width)
        both = jnp.dot(block, module_q[...], preferred_element_type=f32)
        glu = (both[:, :channels] * jax.nn.sigmoid(both[:, channels:])).astype(bf16)
        padded[k, pl.ds(pad, 2 * length), :] = glu.astype(f32)

    channels_at = pl.ds(pl.multiple_of(m.quarter * channels, channels), channels)
    conv_rows = 64

    def convolve(k, _):
        for first in range(0, 2 * length, conv_rows):
            conved = jnp.zeros((conv_rows, channels), f32)
            for t in range(kernel):
                shifted = padded[k, pl.ds(first + t + pad - kernel // 2, conv_rows), :]
                conved = conved + shifted * taps[pl.ds(t, 1), channels_at]
            gains = head_gain[:, channels_at]
            for g in range(0, channels, HEAD_DIM):
                grouped = conved[:, g : g + HEAD_DIM]
                head_mean = jnp.mean(grouped, axis=-1, keepdims=True)
                head_var = jnp.mean(jnp.square(grouped - head_mean), axis=-1, keepdims=True)
                scaled = (grouped - head_mean) * lax.rsqrt(head_var + group_eps) * gains[:, g : g + HEAD_DIM]
                activated[k, pl.ds(first, conv_rows), pl.ds(g, HEAD_DIM)] = jax.nn.silu(scaled).astype(bf16)
        return _

    for k in range(4):
        gather.ready(k)
        gated(k)
    lax.fori_loop(0, 4, convolve, 0)
    m.arrived(OUT)

    def columns(weight, c):
        slots = tile // weight.shape[2]
        return jnp.concatenate([weight[c * slots + i] for i in range(slots)], axis=1)

    def tile_loop(step):
        def run(c, _):
            step(columns(out_q, c), pl.ds(pl.multiple_of(c * tile, tile), tile))
            return _

        lax.fori_loop(0, width // tile, run, 0)

    def phase_columns(phase):
        if phase == 0:
            return slice(None)
        size = 2 * width // n_fs
        owner = (m.place + m.ring + 1 - phase) % m.ring
        return pl.ds(pl.multiple_of(owner * size, size), size)

    def for_columns(phase, step):
        if phase == 0:
            tile_loop(step)
        else:
            owner = ((m.place + m.ring + 1 - phase) % m.ring) * 2
            weight = jnp.concatenate([down_q[owner], down_q[owner + 1]], axis=1)
            step(weight, phase_columns(phase))

    def tp_copy(phase, k):
        b, at = min(phase, 1), phase_columns(phase)
        phase_sems = (sum_send.at[phase], sum_recv.at[phase])
        return m.copy(tp_out.at[b, k, :, at], tp_in.at[b, k, :, at], m.to_tp, phase_sems, k)

    def x_copy(phase, k, low):
        b, columns_at = min(phase, 1), phase_columns(phase)
        at = pl.ds(0, length // 2) if low else pl.ds(length // 2, length // 2)
        to_rep = k == 2 or (k == 3 and low)
        return m.copy(
            x_out.at[b, k - 1, at, columns_at],
            x_in.at[b, k - 1, at, columns_at],
            m.peers[2 if to_rep else 1],
            (sum_send.at[phase], sum_recv.at[phase]),
            2 * k + 2 + low,
        )

    def far_sums(phase, far):
        b = min(phase, 1)
        for k in (3, 2, 1, 0):

            def step(weight, at):
                product = jnp.dot(far(k), weight, preferred_element_type=f32)
                tp_out[b, k, :, at] = product.astype(bf16)

            for_columns(phase, step)
            tp_copy(phase, k).start()

    def near_sums(phase, near):
        b = min(phase, 1)
        for k in (3, 2, 1, 0):
            tp_copy(phase, k).wait_recv()

            def step(weight, at):
                part = jnp.dot(near(k), weight, preferred_element_type=f32)
                part = part + tp_in[b, k, :, at].astype(f32)
                if k == 0:
                    total[b, :, at] = part
                else:
                    x_out[b, k - 1, :, at] = part.astype(bf16)

            for_columns(phase, step)
            if k == 3:
                x_copy(phase, 3, 1).start()
                x_copy(phase, 3, 0).start()
            elif k:
                x_copy(phase, k, k - 1).start()

    def forward_sums(phase):
        b, columns_at = min(phase, 1), phase_columns(phase)
        for k, low in ((1, 1), (2, 0)):
            x_copy(phase, 3, low).wait_recv()
            first = 0 if low else length // 2

            def add(i, _):
                at = pl.ds(pl.multiple_of(first + i * high, high), high)
                part = x_out[b, k - 1, at, columns_at].astype(f32)
                part = part + x_in[b, 2, at, columns_at].astype(f32)
                x_out[b, k - 1, at, columns_at] = part.astype(bf16)
                return _

            lax.fori_loop(0, length // (2 * high), add, 0)
            x_copy(phase, k, low).start()

    def sums_arrived(phase):
        for k in (1, 2):
            for low in (0, 1):
                x_copy(phase, k, low).wait_recv()

    def all_sums(b, at):
        part = total[b, at, :]
        for k in (1, 2):
            part = part + x_in[b, k - 1, at, :].astype(f32)
        return part

    far_sums(0, lambda k: activated[k, far_at, :])
    for w in (FFN_GATE, FFN_UP):
        m.push(w, 1, 1)
    near_sums(0, lambda k: activated[k, near_at, :])
    for w in (FFN_GATE, FFN_UP):
        m.push(w, 0, 2)
    forward_sums(0)
    for w in (FFN_GATE, FFN_UP):
        m.push(w, 1, 2)
    m.pair_copy(DOWN).start()
    sums_arrived(0)

    def norm_rows(i, _):
        at = pl.ds(pl.multiple_of(i * high, high), high)
        mid = (tokens[at, :].astype(f32) + all_sums(0, at)).astype(bf16)
        middle[at, :] = mid
        rows[m.tp, at, :] = rms_scale(mid.astype(f32), ffn_gain[...]).astype(bf16)
        return _

    lax.fori_loop(0, length // high, norm_rows, 0)
    ffn_gather = RowGather(m, rows.at[m.tp], rows, row_sems)
    ffn_gather.start()
    for s in range(3, m.ring):
        for p in (0, 1):
            for w in (FFN_GATE, FFN_UP):
                m.push(w, p, s)
            if s == 3 and p == 0:
                ffn_gather.forward()
    if m.ring < 4:
        ffn_gather.forward()
    for p in (0, 1):
        m.push(DOWN, p, 1)
    ffn_gather.finish()
    for k in range(4):
        ffn_gather.ready(k)
    m.arrived(FFN_GATE)
    m.arrived(FFN_UP)

    def feed(i, _):
        at = pl.ds(2 * i, 2)
        block = rows[at].reshape(2 * length, width)
        both = jnp.dot(block, ffn_q[...], preferred_element_type=f32)
        hidden[at] = (jax.nn.silu(both[:, :units]) * both[:, units:]).astype(bf16).reshape(2, length, -1)
        return _

    lax.fori_loop(0, 4, feed, 0)
    for t in range(m.ring):
        if t and t == m.ring - 1:
            m.arrived(DOWN)
        elif t:
            for p in (0, 1):
                m.push(DOWN, p, t + 1)
        far_sums(1 + t, lambda k: hidden[2 * k + 1 - m.tp])
        near_sums(1 + t, lambda k: hidden[2 * k + m.tp])
        if t:
            forward_sums(t)
    forward_sums(m.ring)
    for t in range(m.ring):
        sums_arrived(1 + t)

    def finish(i, _):
        at = pl.ds(pl.multiple_of(i * high, high), high)
        finished[at, :] = (middle[at, :].astype(f32) + all_sums(1, at)).astype(bf16)
        return _

    lax.fori_loop(0, length // high, finish, 0)
    leave = pltpu.make_async_copy(finished, result, local_sem.at[17])
    leave.start()
    gather.sent()
    ffn_gather.sent()
    for phase in range(1 + m.ring):
        for k in range(4):
            tp_copy(phase, k).wait_send()
        for k in (1, 2, 3):
            for low in (0, 1):
                x_copy(phase, k, low).wait_send()
    m.sent()
    leave.wait()


def body(
    tokens,
    mix_gain,
    value_weight,
    gate_weight,
    conv_taps,
    head_gain,
    out_weight,
    ffn_gain,
    ffn_gate_weight,
    ffn_up_weight,
    down_weight,
):
    n_rep, n_fs, n_tp = lax.axis_size("rep"), lax.axis_size("fs"), lax.axis_size("tp")
    length, seq_count, width = tokens.shape
    assert n_rep == 2 and n_tp == 2 and n_fs % 2 == 0 and n_fs > 4 and seq_count == 1
    ring = n_fs // 2
    kernel = conv_taps.shape[0]
    channels, units = out_weight.shape[0] // 4, down_weight.shape[0] // 4
    pad = -(-(kernel // 2) // 8) * 8
    sem = pltpu.SemaphoreType.DMA
    weights = (value_weight, gate_weight, out_weight, ffn_gate_weight, ffn_up_weight, down_weight)
    operands = (
        tokens.reshape(length, width),
        mix_gain.reshape(1, width),
        value_weight,
        gate_weight,
        conv_taps,
        head_gain.reshape(1, -1),
        out_weight,
        ffn_gain.reshape(1, width),
        ffn_gate_weight,
        ffn_up_weight,
        down_weight,
    )
    layer_rows = pl.pallas_call(
        functools.partial(layer_kernel, n_rep, n_fs),
        out_shape=jax.ShapeDtypeStruct((length, width), bf16),
        in_specs=[pl.BlockSpec(memory_space=pl.ANY)] * len(operands),
        out_specs=pl.BlockSpec(memory_space=pl.ANY),
        scratch_shapes=[pltpu.VMEM(w.shape, bf16) for w in weights]
        + [
            pltpu.VMEM((width, 2 * channels), bf16),
            pltpu.VMEM((n_fs, channels, out_weight.shape[1]), bf16),
            pltpu.VMEM((width, 2 * units), bf16),
            pltpu.VMEM((n_fs, units, down_weight.shape[1]), bf16),
            pltpu.VMEM((length, width), bf16),
            pltpu.VMEM((1, width), f32),
            pltpu.VMEM(conv_taps.shape, f32),
            pltpu.VMEM((1, head_gain.shape[0]), f32),
            pltpu.VMEM((1, width), f32),
            pltpu.VMEM((8, length, width), bf16),
            pltpu.VMEM((8, length, width), bf16),
            pltpu.VMEM((4, 2 * length + 2 * pad, channels), f32),
            pltpu.VMEM((4, 2 * length, channels), bf16),
            pltpu.VMEM((8, length, units), bf16),
            pltpu.VMEM((length, width), bf16),
            pltpu.VMEM((2, length, width), f32),
            pltpu.VMEM((2, 4, length, width), bf16),
            pltpu.VMEM((2, 4, length, width), bf16),
            pltpu.VMEM((2, 3, length, width), bf16),
            pltpu.VMEM((2, 3, length, width), bf16),
            pltpu.VMEM((length, width), bf16),
        ]
        + [sem((6, 2, ring - 1)), sem((6, 2, ring - 1)), sem((6,)), sem((6,))]
        + [sem((11,)), sem((11,)), sem((11,)), sem((11,))]
        + [sem((1 + ring, 10)), sem((1 + ring, 10)), sem((18,))],
        compiler_params=pltpu.CompilerParams(
            collective_id=0, has_side_effects=True, vmem_limit_bytes=60 * 1024 * 1024
        ),
    )(*operands)
    return layer_rows.reshape(length, seq_count, width)


def solution(mesh):
    placed = (
        P("tp", ("rep", "fs"), None),
        P(),
        P("fs", "tp"),
        P("fs", "tp"),
        P(None, "tp"),
        P("tp"),
        P("tp", "fs"),
        P(),
        P("fs", "tp"),
        P("fs", "tp"),
        P("tp", "fs"),
    )
    return jax.shard_map(
        body, mesh=mesh, in_specs=placed, out_specs=P("tp", ("rep", "fs"), None), check_vma=False
    )
```

```python
import functools

import jax
import jax.numpy as jnp
from jax import lax
from jax.experimental import pallas as pl
from jax.experimental.pallas import tpu as pltpu
from jax.sharding import PartitionSpec as P

HEAD_DIM = 128
MESH = pl.DeviceIdType.MESH

norm_eps = 1e-06
group_eps = 1e-05
f32 = jnp.float32
bf16 = jnp.bfloat16


def rms_scale(matrix, scales):
    return matrix * lax.rsqrt(jnp.mean(matrix * matrix, axis=-1, keepdims=True) + norm_eps) * scales


MODULE, OUT, FFN, DOWN = range(4)


class Moves:
    def __init__(self, n_rep, n_fs, sources, wholes, axes, sems):
        self.rep, self.fs, self.tp = lax.axis_index("rep"), lax.axis_index("fs"), lax.axis_index("tp")
        rep, fs, tp = self.rep, self.fs, self.tp
        self.n_fs, self.ring = n_fs, n_fs // 2
        self.pair, self.place = fs % 2, fs // 2
        flip = fs + 1 - 2 * self.pair
        self.to_tp = (rep, fs, 1 - tp)
        self.peers = (None, (rep, flip, tp), (1 - rep, fs, tp), (1 - rep, flip, tp))
        self.after = (rep, (fs + 2) % n_fs, tp)
        self.before = (rep, (fs + n_fs - 2) % n_fs, tp)
        self.quarter = rep * 2 + self.pair
        self.other = rep * 2 + 1 - self.pair
        self.sources, self.wholes, self.axes = sources, wholes, axes
        self.send, self.ring_recv, self.pair_recv = sems

    def greet(self):
        for device in self.peers[1:] + (self.to_tp, self.after, self.before):
            pl.semaphore_signal(pltpu.get_barrier_semaphore(), inc=1, device_id=device, device_id_type=MESH)

    def meet(self):
        pl.semaphore_wait(pltpu.get_barrier_semaphore(), 6)

    def part(self, w, quarter):
        size = self.sources[w].shape[self.axes[w]] // 4
        at = pl.ds(pl.multiple_of(quarter * size, size), size)
        return (slice(None), at) if self.axes[w] == 1 else (at, slice(None))

    def slots(self, w, owner, count=1):
        if self.axes[w] == 0:
            return (owner,) if count == 1 else (pl.ds(owner, count),)
        size = self.sources[w].shape[0]
        return (pl.ds(pl.multiple_of(owner * size, size), count * size), slice(None))

    def copy(self, src, dst, device, send_sem, recv_sem):
        return pltpu.make_async_remote_copy(
            src_ref=src,
            dst_ref=dst,
            send_sem=send_sem,
            recv_sem=recv_sem,
            device_id=device,
            device_id_type=MESH,
        )

    def pair_copy(self, w):
        source, there = self.sources[w].at[self.part(w, self.other)], self.wholes[w].at[self.slots(w, self.fs)]
        return self.copy(source, there, self.peers[1], self.send.at[w], self.pair_recv.at[w])

    def ring_copy(self, w, p, s):
        parity = p if w == DOWN else self.pair if p == 0 else 1 - self.pair
        owner = ((self.place + self.ring + 1 - s) % self.ring) * 2 + parity
        there = self.wholes[w].at[self.slots(w, owner)]
        here = self.sources[w].at[self.part(w, self.quarter)] if w != DOWN and s == 1 and p == 0 else there
        return self.copy(here, there, self.after, self.send.at[w], self.ring_recv.at[w, p, s - 1])

    def push(self, w, p, s):
        if s > 1:
            self.ring_copy(w, p, s - 1).wait_recv()
        elif p == (0 if w == DOWN else 1):
            self.pair_copy(w).wait_recv()
        self.ring_copy(w, p, s).start()

    def arrived(self, w):
        for p in (0, 1):
            self.ring_copy(w, p, self.ring - 1).wait_recv()

    def sent(self, w):
        all_sent = self.wholes[w].at[self.slots(w, 0, self.n_fs - 1)]
        self.copy(all_sent, all_sent, self.after, self.send.at[w], self.pair_recv.at[w]).wait_send()


class RowGather:
    def __init__(self, m, rows, send_sem, recv_sems):
        half = rows.shape[1] // 2
        low, high = pl.ds(0, half), pl.ds(half, half)
        _, pair, rep, _ = m.peers
        first, near_pair, near_rep, across = (2 * k + m.tp for k in range(4))
        moves = (
            (rows.at[first, low], rows.at[near_rep, low], rep),
            (rows.at[first, high], rows.at[near_pair, high], pair),
            (rows.at[first, high], rows.at[near_rep, high], rep),
            (rows.at[first, low], rows.at[near_pair, low], pair),
            (rows.at[near_rep, low], rows.at[across, low], pair),
            (rows.at[near_pair, high], rows.at[across, high], rep),
            (rows.at[first], rows.at[first], m.to_tp),
            (rows.at[near_rep], rows.at[near_rep], m.to_tp),
            (rows.at[near_pair], rows.at[near_pair], m.to_tp),
            (rows.at[across, low], rows.at[across, low], m.to_tp),
            (rows.at[across, high], rows.at[across, high], m.to_tp),
        )
        self.copies = [m.copy(*move, send_sem, recv_sems.at[i]) for i, move in enumerate(moves)]
        seven = rows.at[pl.ds(0, 7)]
        self.all_sent = m.copy(seven, seven, pair, send_sem, recv_sems.at[0])

    def start(self):
        for i in (0, 1, 2, 3, 6):
            self.copies[i].start()

    def forward(self):
        for i in (0, 1):
            self.copies[i].wait_recv()
            self.copies[i + 4].start()

    def finish(self):
        for i in (2, 3, 4, 5):
            self.copies[i].wait_recv()
            self.copies[i + 5].start()

    def ready(self, k):
        for i in ((6,), (8,), (7,), (9, 10))[k]:
            self.copies[i].wait_recv()

    def sent(self):
        self.all_sent.wait_send()


def layer_kernel(
    n_rep, n_fs, tokens_in, mix_gain_in, value, gate, taps_in, head_gain_in, out, ffn_gain_in, ffn_gate, ffn_up,
    down, result,
    *scratch,
):
    staged, wholes, scratch = scratch[:4], scratch[4:8], scratch[8:]
    module_q, out_q, ffn_q, down_q = wholes
    tokens, mix_gain, taps, head_gain, ffn_gain = scratch[:5]
    rows_a, rows, padded, activated, hidden, middle, total, tp_out, tp_in, x_out, x_in, finished = scratch[5:17]
    weight_sems, scratch = scratch[17:20], scratch[20:]
    row_send, row_recv, tp_send, tp_recv, x_send, x_first, x_last, stage_sem, place_sem, small_sem, end_sem = scratch
    channels, units = out_q.shape[1], down_q.shape[1]
    m = Moves(n_rep, n_fs, staged, wholes, (1, 0, 1, 0), weight_sems)
    length, width = tokens.shape
    kernel = taps.shape[0]
    pad = (padded.shape[1] - 2 * length) // 2
    tile = 512
    high = 32
    near_at = pl.ds(pl.multiple_of(m.tp * length, length), length)
    far_at = pl.ds(pl.multiple_of((1 - m.tp) * length, length), length)

    def stage(w, shards):
        if len(shards) == 1:
            pltpu.make_async_copy(shards[0], staged[w], stage_sem.at[w]).start()
            return
        size = shards[0].shape[1] // 4
        for i, shard in enumerate(shards):
            for q in range(4):
                there = staged[w].at[:, pl.ds((2 * q + i) * size, size)]
                pltpu.make_async_copy(shard.at[:, pl.ds(q * size, size)], there, stage_sem.at[w]).start()

    def stage_wait(w):
        pltpu.make_async_copy(staged[w], staged[w], stage_sem.at[w]).wait()

    def place(w, wait):
        there = wholes[w].at[m.slots(w, m.fs)]
        copy = pltpu.make_async_copy(staged[w].at[m.part(w, m.quarter)], there, place_sem.at[w])
        copy.wait() if wait else copy.start()

    smalls = ((tokens_in, tokens), (mix_gain_in, mix_gain), (taps_in, taps))
    smalls += ((head_gain_in, head_gain), (ffn_gain_in, ffn_gain))
    small = [pltpu.make_async_copy(s, d, small_sem.at[i]) for i, (s, d) in enumerate(smalls)]
    m.greet()
    stage(MODULE, (value, gate))
    stage(OUT, (out,))
    small[0].start()
    small[1].start()
    stage(FFN, (ffn_gate, ffn_up))
    stage(DOWN, (down,))
    for copy in small[2:]:
        copy.start()
    stage_wait(MODULE)
    m.meet()
    m.pair_copy(MODULE).start()
    m.push(MODULE, 0, 1)
    stage_wait(OUT)
    m.pair_copy(OUT).start()
    m.push(OUT, 0, 1)

    def module_norm(i, _):
        at = pl.ds(pl.multiple_of(i * high, high), high)
        rows_a[m.tp, at, :] = rms_scale(tokens[at, :].astype(f32), mix_gain[...]).astype(bf16)
        return _

    small[0].wait()
    small[1].wait()
    lax.fori_loop(0, length // high, module_norm, 0)
    gather = RowGather(m, rows_a, row_send, row_recv)
    gather.start()
    m.push(MODULE, 1, 1)
    m.push(OUT, 1, 1)
    for w in (FFN, DOWN):
        stage_wait(w)
    for w in (MODULE, OUT, FFN, DOWN):
        place(w, False)
    zeros = jnp.zeros((4, pad, channels), f32)
    padded[:, pl.ds(0, pad), :] = zeros
    padded[:, pl.ds(pad + 2 * length, pad), :] = zeros
    for s in range(2, m.ring):
        for p in (0, 1):
            m.push(MODULE, p, s)
            m.push(OUT, p, s)
            if s == 2 and p == 0:
                gather.forward()
    m.pair_copy(FFN).start()
    m.push(FFN, 0, 1)
    gather.finish()
    for w in (MODULE, OUT, FFN, DOWN):
        place(w, True)
    for copy in small[2:]:
        copy.wait()
    m.arrived(MODULE)

    def gated(k):
        block = rows_a[pl.ds(2 * k, 2)].reshape(2 * length, width)
        both = jnp.dot(block, module_q[...], preferred_element_type=f32)
        glu = (both[:, :channels] * jax.nn.sigmoid(both[:, channels:])).astype(bf16)
        padded[k, pl.ds(pad, 2 * length), :] = glu.astype(f32)

    channels_at = pl.ds(pl.multiple_of(m.quarter * channels, channels), channels)
    conv_rows = 64

    def convolve(k, _):
        for first in range(0, 2 * length, conv_rows):
            conved = jnp.zeros((conv_rows, channels), f32)
            for t in range(kernel):
                shifted = padded[k, pl.ds(first + t + pad - kernel // 2, conv_rows), :]
                conved = conved + shifted * taps[pl.ds(t, 1), channels_at]
            gains = head_gain[:, channels_at]
            for g in range(0, channels, HEAD_DIM):
                grouped = conved[:, g : g + HEAD_DIM]
                head_mean = jnp.mean(grouped, axis=-1, keepdims=True)
                head_var = jnp.mean(jnp.square(grouped - head_mean), axis=-1, keepdims=True)
                scaled = (grouped - head_mean) * lax.rsqrt(head_var + group_eps) * gains[:, g : g + HEAD_DIM]
                activated[k, pl.ds(first, conv_rows), pl.ds(g, HEAD_DIM)] = jax.nn.silu(scaled).astype(bf16)
        return _

    for k in range(4):
        gather.ready(k)
        gated(k)
    lax.fori_loop(0, 4, convolve, 0)
    m.push(FFN, 1, 1)
    m.arrived(OUT)

    def columns(weight, c):
        slots = tile // weight.shape[2]
        return jnp.concatenate([weight[c * slots + i] for i in range(slots)], axis=1)

    def tile_loop(step):
        def run(c, _):
            step(columns(out_q, c), pl.ds(pl.multiple_of(c * tile, tile), tile))
            return _

        lax.fori_loop(0, width // tile, run, 0)

    size = down_q.shape[2]
    halved = size % 128 == 0
    phases = [None] + [(t, None) for t in range(m.ring - 1)]
    phases += [(m.ring - 1, 0), (m.ring - 1, 1)] if halved else [(m.ring - 1, None)]

    def phase_owner(phase):
        t, p = phases[phase]
        base = ((m.place + m.ring - t) % m.ring) * 2
        if p is None:
            return base, 2
        return base + p, 1

    def phase_columns(phase):
        if phase == 0:
            return slice(None)
        owner, count = phase_owner(phase)
        return pl.ds(pl.multiple_of(owner * size, count * size), count * size)

    def for_columns(phase, step):
        if phase == 0:
            tile_loop(step)
        else:
            owner, count = phase_owner(phase)
            weight = jnp.concatenate([down_q[owner + i] for i in range(count)], axis=1)
            step(weight, phase_columns(phase))

    def tp_copy(phase, k, count=1):
        b, at = min(phase, 1), (pl.ds(k, count), slice(None), phase_columns(phase))
        recv_sem = tp_recv.at[phase, 0 if k == 3 else 1]
        return m.copy(tp_out.at[(b, *at)], tp_in.at[(b, *at)], m.to_tp, tp_send.at[b], recv_sem)

    def x_copy(phase, k, low):
        b, columns_at = min(phase, 1), phase_columns(phase)
        at = pl.ds(0, length // 2) if low else pl.ds(length // 2, length // 2)
        to_rep = k == 2 or (k == 3 and low)
        there = (b, k - 1, at, columns_at)
        recv_sem = x_first.at[phase, low] if k == 3 else x_last.at[b]
        return m.copy(x_out.at[there], x_in.at[there], m.peers[2 if to_rep else 1], x_send.at[b], recv_sem)

    def far_sums(phase, far):
        b = min(phase, 1)
        for k in (3, 2, 1, 0):

            def step(weight, at):
                product = jnp.dot(far(k), weight, preferred_element_type=f32)
                tp_out[b, k, :, at] = product.astype(bf16)

            for_columns(phase, step)
            tp_copy(phase, k).start()

    def near_sums(phase, near):
        b = min(phase, 1)
        for k in (3, 2, 1, 0):
            if k == 3:
                tp_copy(phase, 3).wait_recv()
            elif k == 2:
                tp_copy(phase, 0, 3).wait_recv()

            def step(weight, at):
                part = jnp.dot(near(k), weight, preferred_element_type=f32)
                part = part + tp_in[b, k, :, at].astype(f32)
                if k == 0:
                    total[b, :, at] = part
                else:
                    x_out[b, k - 1, :, at] = part.astype(bf16)

            for_columns(phase, step)
            if k == 3:
                x_copy(phase, 3, 1).start()
                x_copy(phase, 3, 0).start()
            elif k:
                x_copy(phase, k, k - 1).start()

    def forward_sums(phase):
        b, columns_at = min(phase, 1), phase_columns(phase)
        for k, low in ((1, 1), (2, 0)):
            x_copy(phase, 3, low).wait_recv()
            first = 0 if low else length // 2

            def add(i, _):
                at = pl.ds(pl.multiple_of(first + i * high, high), high)
                part = x_out[b, k - 1, at, columns_at].astype(f32)
                part = part + x_in[b, 2, at, columns_at].astype(f32)
                x_out[b, k - 1, at, columns_at] = part.astype(bf16)
                return _

            lax.fori_loop(0, length // (2 * high), add, 0)
            x_copy(phase, k, low).start()

    def sums_arrived(b):
        both = x_in.at[b, pl.ds(0, 2)]
        m.copy(both, both, m.peers[1], x_send.at[b], x_last.at[b]).wait_recv()

    def sums_sent(b):
        m.copy(tp_out.at[b], tp_out.at[b], m.to_tp, tp_send.at[b], x_last.at[b]).wait_send()
        m.copy(x_out.at[b], x_out.at[b], m.peers[1], x_send.at[b], x_last.at[b]).wait_send()

    def all_sums(b, at):
        part = total[b, at, :]
        for k in (1, 2):
            part = part + x_in[b, k - 1, at, :].astype(f32)
        return part

    far_sums(0, lambda k: activated[k, far_at, :])
    near_sums(0, lambda k: activated[k, near_at, :])
    m.push(FFN, 0, 2)
    forward_sums(0)
    m.push(FFN, 1, 2)
    m.pair_copy(DOWN).start()
    gather.sent()
    sums_arrived(0)

    def norm_rows(i, _):
        at = pl.ds(pl.multiple_of(i * high, high), high)
        mid = (tokens[at, :].astype(f32) + all_sums(0, at)).astype(bf16)
        middle[at, :] = mid
        rows[m.tp, at, :] = rms_scale(mid.astype(f32), ffn_gain[...]).astype(bf16)
        return _

    lax.fori_loop(0, length // high, norm_rows, 0)
    gather = RowGather(m, rows, row_send, row_recv)
    gather.start()
    for s in range(3, m.ring):
        for p in (0, 1):
            m.push(FFN, p, s)
            if s == 3 and p == 0:
                gather.forward()
    if m.ring < 4:
        gather.forward()
    for p in (0, 1):
        m.push(DOWN, p, 1)
    gather.finish()
    for k in range(4):
        gather.ready(k)
    m.arrived(FFN)

    def feed(i, _):
        at = pl.ds(2 * i, 2)
        block = rows[at].reshape(2 * length, width)
        both = jnp.dot(block, ffn_q[...], preferred_element_type=f32)
        hidden[at] = (jax.nn.silu(both[:, :units]) * both[:, units:]).astype(bf16).reshape(2, length, -1)
        return _

    lax.fori_loop(0, 4, feed, 0)
    m.push(DOWN, 0, 2)
    for phase in range(1, len(phases)):
        t, p = phases[phase]
        for q in (0, 1) if p is None else (p,):
            if t == m.ring - 1:
                m.ring_copy(DOWN, q, t).wait_recv()
            elif t and (t, q) != (1, 0):
                m.push(DOWN, q, t + 1)
        far_sums(phase, lambda k: hidden[2 * k + 1 - m.tp])
        near_sums(phase, lambda k: hidden[2 * k + m.tp])
        if phase > 1:
            forward_sums(phase - 1)
    forward_sums(len(phases) - 1)
    sums_arrived(1)

    def finish(i, _):
        at = pl.ds(pl.multiple_of(i * high, high), high)
        finished[at, :] = (middle[at, :].astype(f32) + all_sums(1, at)).astype(bf16)
        return _

    lax.fori_loop(0, length // high, finish, 0)
    leave = pltpu.make_async_copy(finished, result, end_sem)
    leave.start()
    gather.sent()
    for b in (0, 1):
        sums_sent(b)
    for w in (MODULE, OUT, FFN, DOWN):
        m.sent(w)
    leave.wait()


def body(
    tokens,
    mix_gain,
    value_weight,
    gate_weight,
    conv_taps,
    head_gain,
    out_weight,
    ffn_gain,
    ffn_gate_weight,
    ffn_up_weight,
    down_weight,
):
    n_rep, n_fs, n_tp = lax.axis_size("rep"), lax.axis_size("fs"), lax.axis_size("tp")
    length, seq_count, width = tokens.shape
    assert n_rep == 2 and n_tp == 2 and n_fs % 2 == 0 and n_fs > 4 and seq_count == 1
    ring = n_fs // 2
    kernel = conv_taps.shape[0]
    channels, units = out_weight.shape[0] // 4, down_weight.shape[0] // 4
    pad = -(-(kernel // 2) // 8) * 8
    sem = pltpu.SemaphoreType.DMA
    operands = (
        tokens.reshape(length, width),
        mix_gain.reshape(1, width),
        value_weight,
        gate_weight,
        conv_taps,
        head_gain.reshape(1, -1),
        out_weight,
        ffn_gain.reshape(1, width),
        ffn_gate_weight,
        ffn_up_weight,
        down_weight,
    )
    layer_rows = pl.pallas_call(
        functools.partial(layer_kernel, n_rep, n_fs),
        out_shape=jax.ShapeDtypeStruct((length, width), bf16),
        in_specs=[pl.BlockSpec(memory_space=pl.ANY)] * len(operands),
        out_specs=pl.BlockSpec(memory_space=pl.ANY),
        scratch_shapes=[
            pltpu.VMEM((value_weight.shape[0], 8 * channels), bf16),
            pltpu.VMEM(out_weight.shape, bf16),
            pltpu.VMEM((ffn_gate_weight.shape[0], 8 * units), bf16),
            pltpu.VMEM(down_weight.shape, bf16),
            pltpu.VMEM((width, 2 * channels), bf16),
            pltpu.VMEM((n_fs, channels, out_weight.shape[1]), bf16),
            pltpu.VMEM((width, 2 * units), bf16),
            pltpu.VMEM((n_fs, units, down_weight.shape[1]), bf16),
            pltpu.VMEM((length, width), bf16),
            pltpu.VMEM((1, width), f32),
            pltpu.VMEM(conv_taps.shape, f32),
            pltpu.VMEM((1, head_gain.shape[0]), f32),
            pltpu.VMEM((1, width), f32),
            pltpu.VMEM((8, length, width), bf16),
            pltpu.VMEM((8, length, width), bf16),
            pltpu.VMEM((4, 2 * length + 2 * pad, channels), f32),
            pltpu.VMEM((4, 2 * length, channels), bf16),
            pltpu.VMEM((8, length, units), bf16),
            pltpu.VMEM((length, width), bf16),
            pltpu.VMEM((2, length, width), f32),
            pltpu.VMEM((2, 4, length, width), bf16),
            pltpu.VMEM((2, 4, length, width), bf16),
            pltpu.VMEM((2, 3, length, width), bf16),
            pltpu.VMEM((2, 3, length, width), bf16),
            pltpu.VMEM((length, width), bf16),
        ]
        + [sem((4,)), sem((4, 2, ring - 1)), sem((4,))]
        + [sem, sem((11,)), sem((2,)), sem((ring + 2, 2)), sem((2,)), sem((ring + 2, 2)), sem((2,))]
        + [sem((4,)), sem((4,)), sem((5,)), sem],
        compiler_params=pltpu.CompilerParams(
            collective_id=0, has_side_effects=True, vmem_limit_bytes=60 * 1024 * 1024
        ),
    )(*operands)
    return layer_rows.reshape(length, seq_count, width)


def solution(mesh):
    placed = (
        P("tp", ("rep", "fs"), None),
        P(),
        P("fs", "tp"),
        P("fs", "tp"),
        P(None, "tp"),
        P("tp"),
        P("tp", "fs"),
        P(),
        P("fs", "tp"),
        P("fs", "tp"),
        P("tp", "fs"),
    )
    return jax.shard_map(
        body, mesh=mesh, in_specs=placed, out_specs=P("tp", ("rep", "fs"), None), check_vma=False
    )
```

```python
import functools

import jax
import jax.numpy as jnp
from jax import lax
from jax.experimental import pallas as pl
from jax.experimental.pallas import tpu as pltpu
from jax.sharding import PartitionSpec as P

HEAD_DIM = 128
MESH = pl.DeviceIdType.MESH

norm_eps = 1e-06
group_eps = 1e-05
f32 = jnp.float32
bf16 = jnp.bfloat16


def rms_scale(matrix, scales):
    return matrix * lax.rsqrt(jnp.mean(matrix * matrix, axis=-1, keepdims=True) + norm_eps) * scales


MODULE, OUT, FFN, DOWN = range(4)


class Moves:
    def __init__(self, n_rep, n_fs, sources, wholes, axes, sems):
        self.rep, self.fs, self.tp = lax.axis_index("rep"), lax.axis_index("fs"), lax.axis_index("tp")
        rep, fs, tp = self.rep, self.fs, self.tp
        self.n_fs, self.ring = n_fs, n_fs // 2
        self.pair, self.place = fs % 2, fs // 2
        flip = fs + 1 - 2 * self.pair
        self.to_tp = (rep, fs, 1 - tp)
        self.peers = (None, (rep, flip, tp), (1 - rep, fs, tp), (1 - rep, flip, tp))
        self.after = (rep, (fs + 2) % n_fs, tp)
        self.before = (rep, (fs + n_fs - 2) % n_fs, tp)
        self.quarter = rep * 2 + self.pair
        self.other = rep * 2 + 1 - self.pair
        self.sources, self.wholes, self.axes = sources, wholes, axes
        self.send, self.ring_recv, self.piece_recv, self.pair_recv = sems
        self.pieces = max(1, wholes[DOWN].shape[2] // 128)

    def greet(self):
        for device in self.peers[1:] + (self.to_tp, self.after, self.before):
            pl.semaphore_signal(pltpu.get_barrier_semaphore(), inc=1, device_id=device, device_id_type=MESH)

    def meet(self):
        pl.semaphore_wait(pltpu.get_barrier_semaphore(), 6)

    def part(self, w, quarter):
        size = self.sources[w].shape[self.axes[w]] // 4
        at = pl.ds(pl.multiple_of(quarter * size, size), size)
        return (slice(None), at) if self.axes[w] == 1 else (at, slice(None))

    def slots(self, w, owner, count=1):
        if self.axes[w] == 0:
            return (owner,) if count == 1 else (pl.ds(owner, count),)
        size = self.sources[w].shape[0]
        return (pl.ds(pl.multiple_of(owner * size, size), count * size), slice(None))

    def copy(self, src, dst, device, send_sem, recv_sem):
        return pltpu.make_async_remote_copy(
            src_ref=src,
            dst_ref=dst,
            send_sem=send_sem,
            recv_sem=recv_sem,
            device_id=device,
            device_id_type=MESH,
        )

    def pair_copy(self, w):
        source, there = self.sources[w].at[self.part(w, self.other)], self.wholes[w].at[self.slots(w, self.fs)]
        return self.copy(source, there, self.peers[1], self.send.at[w], self.pair_recv.at[w])

    def piece_copy(self, i):
        columns = self.wholes[DOWN].shape[2] // self.pieces
        owner = ((self.place + 2) % self.ring) * 2 + 1
        there = self.wholes[DOWN].at[owner, :, pl.ds(i * columns, columns)]
        recv_sem = self.piece_recv.at[i]
        return self.copy(there, there, self.after, self.send.at[DOWN], recv_sem)

    def ring_copy(self, w, p, s):
        parity = p if w == DOWN else self.pair if p == 0 else 1 - self.pair
        owner = ((self.place + self.ring + 1 - s) % self.ring) * 2 + parity
        there = self.wholes[w].at[self.slots(w, owner)]
        here = self.sources[w].at[self.part(w, self.quarter)] if w != DOWN and s == 1 and p == 0 else there
        return self.copy(here, there, self.after, self.send.at[w], self.ring_recv.at[w, p, s - 1])

    def push_own_ffn(self, lead):
        rows = self.sources[FFN].shape[0]
        at = pl.ds(0, rows // 4) if lead else pl.ds(rows // 4, rows - rows // 4)
        there = self.wholes[FFN].at[self.slots(FFN, self.fs)].at[at, :]
        here = self.sources[FFN].at[self.part(FFN, self.quarter)].at[at, :]
        self.copy(here, there, self.after, self.send.at[FFN], self.ring_recv.at[FFN, 0, 0]).start()

    def push(self, w, p, s):
        if s > 1:
            self.ring_copy(w, p, s - 1).wait_recv()
        elif p == (0 if w == DOWN else 1):
            self.pair_copy(w).wait_recv()
        if (w, p, s) == (DOWN, 1, self.ring - 1):
            for i in range(self.pieces):
                self.piece_copy(i).start()
        else:
            self.ring_copy(w, p, s).start()

    def arrived(self, w):
        for p in (0, 1):
            self.ring_copy(w, p, self.ring - 1).wait_recv()

    def sent(self, w):
        all_sent = self.wholes[w].at[self.slots(w, 0, self.n_fs - 1)]
        self.copy(all_sent, all_sent, self.after, self.send.at[w], self.pair_recv.at[w]).wait_send()


class RowGather:
    def __init__(self, m, rows, send_sem, recv_sems):
        half = rows.shape[1] // 2
        low, high = pl.ds(0, half), pl.ds(half, half)
        _, pair, rep, _ = m.peers
        first, near_pair, near_rep, across = (2 * k + m.tp for k in range(4))
        moves = (
            (rows.at[first, low], rows.at[near_rep, low], rep),
            (rows.at[first, high], rows.at[near_pair, high], pair),
            (rows.at[first, high], rows.at[near_rep, high], rep),
            (rows.at[first, low], rows.at[near_pair, low], pair),
            (rows.at[near_rep, low], rows.at[across, low], pair),
            (rows.at[near_pair, high], rows.at[across, high], rep),
            (rows.at[first], rows.at[first], m.to_tp),
            (rows.at[near_rep], rows.at[near_rep], m.to_tp),
            (rows.at[near_pair], rows.at[near_pair], m.to_tp),
            (rows.at[across, low], rows.at[across, low], m.to_tp),
            (rows.at[across, high], rows.at[across, high], m.to_tp),
        )
        self.copies = [m.copy(*move, send_sem, recv_sems.at[i]) for i, move in enumerate(moves)]
        seven = rows.at[pl.ds(0, 7)]
        self.all_sent = m.copy(seven, seven, pair, send_sem, recv_sems.at[0])

    def start(self):
        for i in (0, 1, 2, 3, 6):
            self.copies[i].start()

    def forward(self):
        for i in (0, 1):
            self.copies[i].wait_recv()
            self.copies[i + 4].start()

    def finish(self):
        for i in (2, 3, 4, 5):
            self.copies[i].wait_recv()
            self.copies[i + 5].start()

    def ready(self, k):
        for i in ((6,), (8,), (7,), (9, 10))[k]:
            self.copies[i].wait_recv()

    def sent(self):
        self.all_sent.wait_send()


def layer_kernel(
    n_rep, n_fs, tokens_in, mix_gain_in, value, gate, taps_in, head_gain_in, out, ffn_gain_in, ffn_gate, ffn_up,
    down, result,
    *scratch,
):
    staged, wholes, scratch = scratch[:4], scratch[4:8], scratch[8:]
    module_q, out_q, ffn_q, down_q = wholes
    tokens, mix_gain, taps, head_gain, ffn_gain = scratch[:5]
    rows_a, rows, padded, activated, hidden, middle, total, tp_out, tp_in, x_out, x_in, finished = scratch[5:17]
    weight_sems, scratch = scratch[17:21], scratch[21:]
    row_send, row_recv, tp_send, tp_recv, x_send, x_first, x_last, stage_sem, small_sem, end_sem = scratch
    channels, units = out_q.shape[1], down_q.shape[1]
    m = Moves(n_rep, n_fs, staged, wholes, (1, 0, 1, 0), weight_sems)
    length, width = tokens.shape
    kernel = taps.shape[0]
    pad = (padded.shape[1] - 2 * length) // 2
    tile = 512
    high = 32
    near_at = pl.ds(pl.multiple_of(m.tp * length, length), length)
    far_at = pl.ds(pl.multiple_of((1 - m.tp) * length, length), length)

    def stage(w, shards):
        if len(shards) == 1:
            pltpu.make_async_copy(shards[0], staged[w], stage_sem.at[w]).start()
            return
        size = shards[0].shape[1] // 4
        for i, shard in enumerate(shards):
            for q in range(4):
                there = staged[w].at[:, pl.ds((2 * q + i) * size, size)]
                pltpu.make_async_copy(shard.at[:, pl.ds(q * size, size)], there, stage_sem.at[w]).start()

    def stage_wait(w):
        pltpu.make_async_copy(staged[w], staged[w], stage_sem.at[w]).wait()

    def place(w, wait):
        there = wholes[w].at[m.slots(w, m.fs)]
        copy = pltpu.make_async_copy(staged[w].at[m.part(w, m.quarter)], there, stage_sem.at[w])
        copy.wait() if wait else copy.start()

    smalls = ((tokens_in, tokens), (mix_gain_in, mix_gain), (taps_in, taps))
    smalls += ((head_gain_in, head_gain), (ffn_gain_in, ffn_gain))
    small = [pltpu.make_async_copy(s, d, small_sem.at[i]) for i, (s, d) in enumerate(smalls)]
    m.greet()
    stage(MODULE, (value, gate))
    stage(OUT, (out,))
    small[0].start()
    small[1].start()
    stage(FFN, (ffn_gate, ffn_up))
    stage(DOWN, (down,))
    for copy in small[2:]:
        copy.start()
    stage_wait(MODULE)
    m.meet()
    m.pair_copy(MODULE).start()
    m.push(MODULE, 0, 1)
    stage_wait(OUT)
    m.pair_copy(OUT).start()
    m.push(OUT, 0, 1)
    stage_wait(FFN)
    m.push_own_ffn(True)

    def module_norm(i, _):
        at = pl.ds(pl.multiple_of(i * high, high), high)
        rows_a[m.tp, at, :] = rms_scale(tokens[at, :].astype(f32), mix_gain[...]).astype(bf16)
        return _

    small[0].wait()
    small[1].wait()
    lax.fori_loop(0, length // high, module_norm, 0)
    gather = RowGather(m, rows_a, row_send, row_recv)
    gather.start()
    m.push(MODULE, 1, 1)
    stage_wait(DOWN)
    for w in (MODULE, OUT, FFN, DOWN):
        place(w, False)
    zeros = jnp.zeros((4, pad, channels), f32)
    padded[:, pl.ds(0, pad), :] = zeros
    padded[:, pl.ds(pad + 2 * length, pad), :] = zeros
    for s in range(2, m.ring):
        m.push(MODULE, 0, s)
        if s > 2:
            m.push(OUT, 0, s - 1)
        m.push(OUT, 1, s - 1)
        m.push(MODULE, 1, s)
        if s == 2:
            gather.forward()
            m.pair_copy(FFN).start()
    for p in (0, 1):
        m.push(OUT, p, m.ring - 1)
    m.push_own_ffn(False)
    gather.finish()
    for w in (MODULE, OUT, FFN, DOWN):
        place(w, True)
    for copy in small[2:]:
        copy.wait()
    m.arrived(MODULE)

    def gated(k):
        block = rows_a[pl.ds(2 * k, 2)].reshape(2 * length, width)
        both = jnp.dot(block, module_q[...], preferred_element_type=f32)
        glu = (both[:, :channels] * jax.nn.sigmoid(both[:, channels:])).astype(bf16)
        padded[k, pl.ds(pad, 2 * length), :] = glu.astype(f32)

    channels_at = pl.ds(pl.multiple_of(m.quarter * channels, channels), channels)
    conv_rows = 64

    def convolve(k, _):
        for first in range(0, 2 * length, conv_rows):
            conved = jnp.zeros((conv_rows, channels), f32)
            for t in range(kernel):
                shifted = padded[k, pl.ds(first + t + pad - kernel // 2, conv_rows), :]
                conved = conved + shifted * taps[pl.ds(t, 1), channels_at]
            gains = head_gain[:, channels_at]
            for g in range(0, channels, HEAD_DIM):
                grouped = conved[:, g : g + HEAD_DIM]
                head_mean = jnp.mean(grouped, axis=-1, keepdims=True)
                head_var = jnp.mean(jnp.square(grouped - head_mean), axis=-1, keepdims=True)
                scaled = (grouped - head_mean) * lax.rsqrt(head_var + group_eps) * gains[:, g : g + HEAD_DIM]
                activated[k, pl.ds(first, conv_rows), pl.ds(g, HEAD_DIM)] = jax.nn.silu(scaled).astype(bf16)
        return _

    for k in range(4):
        gather.ready(k)
        gated(k)
    m.push(FFN, 1, 1)
    lax.fori_loop(0, 4, convolve, 0)
    m.arrived(OUT)

    def columns(weight, c):
        slots = tile // weight.shape[2]
        return jnp.concatenate([weight[c * slots + i] for i in range(slots)], axis=1)

    def tile_loop(step):
        def run(c, _):
            step(columns(out_q, c), pl.ds(pl.multiple_of(c * tile, tile), tile))
            return _

        lax.fori_loop(0, width // tile, run, 0)

    size = down_q.shape[2]
    last_t = m.ring - 1
    phases = [None] + [(t, 0, 2 * size) for t in range(last_t)]
    if size % 128 == 0:
        phases += [(last_t, 0, size)] + [(last_t, size + c, 128) for c in range(0, size, 128)]
    else:
        phases += [(last_t, 0, 2 * size)]
    final = len(phases) - 1
    direct = [i for i in range(1, final + 1) if phases[i][0] == last_t and (phases[i][1] or i == final)]
    final_count = sum(phases[i][2] for i in direct)

    def phase_base(phase):
        return ((m.place + m.ring - phases[phase][0]) % m.ring) * 2

    def phase_columns(phase):
        if phase == 0:
            return slice(None)
        _, first, count = phases[phase]
        return pl.ds(pl.multiple_of(phase_base(phase) * size + first, count), count)

    def phase_weight(phase):
        _, first, count = phases[phase]
        base = phase_base(phase)
        if count == 2 * size:
            return jnp.concatenate([down_q[base], down_q[base + 1]], axis=1)
        return down_q[base + first // size, :, pl.ds(first % size, count)]

    def tp_copy(phase, k, count=1):
        b, at = min(phase, 1), (pl.ds(k, count), slice(None), phase_columns(phase))
        recv_sem = tp_recv.at[phase % 2, 0 if k == 3 else 1]
        return m.copy(tp_out.at[(b, *at)], tp_in.at[(b, *at)], m.to_tp, tp_send.at[b], recv_sem)

    def x_copy(phase, k, low):
        b, columns_at = min(phase, 1), phase_columns(phase)
        at = pl.ds(0, length // 2) if low else pl.ds(length // 2, length // 2)
        to_rep = k == 2 or (k == 3 and low)
        there = (b, k - 1, at, columns_at)
        recv_sem = x_first.at[phase] if k == 3 else x_last.at[b]
        return m.copy(x_out.at[there], x_in.at[there], m.peers[2 if to_rep else 1], x_send.at[b], recv_sem)

    def direct_copy(phase, k):
        there = (1, k - 1, slice(None), phase_columns(phase))
        return m.copy(x_out.at[there], x_in.at[there], m.peers[k], x_send.at[1], x_last.at[2])

    def received(ref, sem):
        m.copy(ref, ref, m.peers[1], x_send.at[0], sem).wait_recv()

    def far_sums(k):
        def step(weight, at):
            product = jnp.dot(activated[k, far_at, :], weight, preferred_element_type=f32)
            tp_out[0, k, :, at] = product.astype(bf16)

        tile_loop(step)
        tp_copy(0, k).start()

    def near_sums(k):
        def step(weight, at):
            part = jnp.dot(activated[k, near_at, :], weight, preferred_element_type=f32)
            part = part + tp_in[0, k, :, at].astype(f32)
            if k == 0:
                total[0, :, at] = part
            else:
                x_out[0, k - 1, :, at] = part.astype(bf16)

        tile_loop(step)
        if k == 3:
            x_copy(0, 3, 1).start()
            x_copy(0, 3, 0).start()
        elif k:
            x_copy(0, k, k - 1).start()

    def ffn_far_sums(phase):
        _, _, count = phases[phase]
        product = jnp.dot(
            hidden[1 - m.tp].reshape(4 * length, units), phase_weight(phase), preferred_element_type=f32
        )
        tp_out[1, :, :, phase_columns(phase)] = product.astype(bf16).reshape(4, length, count)
        tp_copy(phase, 3).start()
        tp_copy(phase, 0, 3).start()

    def ffn_near_sums(phase):
        at = phase_columns(phase)
        parts = jnp.dot(hidden[m.tp].reshape(4 * length, units), phase_weight(phase), preferred_element_type=f32)
        tp_copy(phase, 3).wait_recv()
        for k in (3, 2, 1, 0):
            if k == 2:
                tp_copy(phase, 0, 3).wait_recv()
            part = parts[k * length : (k + 1) * length] + tp_in[1, k, :, at].astype(f32)
            if k == 0:
                total[1, :, at] = part
                continue
            x_out[1, k - 1, :, at] = part.astype(bf16)
            if phase in direct:
                direct_copy(phase, k).start()
            elif k == 3:
                x_copy(phase, 3, 1).start()
                x_copy(phase, 3, 0).start()
            else:
                x_copy(phase, k, k - 1).start()

    def forward_sums(phase):
        b, columns_at = min(phase, 1), phase_columns(phase)
        received(x_in.at[b, 2, :, columns_at], x_first.at[phase])
        for k, low in ((1, 1), (2, 0)):
            first = 0 if low else length // 2

            def add(i, _):
                at = pl.ds(pl.multiple_of(first + i * high, high), high)
                part = x_out[b, k - 1, at, columns_at].astype(f32)
                part = part + x_in[b, 2, at, columns_at].astype(f32)
                x_out[b, k - 1, at, columns_at] = part.astype(bf16)
                return _

            lax.fori_loop(0, length // (2 * high), add, 0)
            x_copy(phase, k, low).start()

    def sums_sent(b):
        m.copy(tp_out.at[b], tp_out.at[b], m.to_tp, tp_send.at[b], x_last.at[b]).wait_send()
        m.copy(x_out.at[b], x_out.at[b], m.peers[1], x_send.at[b], x_last.at[b]).wait_send()

    def all_sums(b, at):
        part = total[b, at, :]
        for k in (1, 2):
            part = part + x_in[b, k - 1, at, :].astype(f32)
        return part

    far_sums(3)
    far_sums(2)
    tp_copy(0, 3).wait_recv()
    near_sums(3)
    far_sums(1)
    far_sums(0)
    tp_copy(0, 0, 3).wait_recv()
    for k in (2, 1, 0):
        near_sums(k)
    m.push(FFN, 0, 2)
    forward_sums(0)
    m.push(FFN, 1, 2)
    m.pair_copy(DOWN).start()
    gather.sent()
    received(x_in.at[0, pl.ds(0, 2)], x_last.at[0])

    def norm_rows(i, _):
        at = pl.ds(pl.multiple_of(i * high, high), high)
        mid = (tokens[at, :].astype(f32) + all_sums(0, at)).astype(bf16)
        middle[at, :] = mid
        rows[m.tp, at, :] = rms_scale(mid.astype(f32), ffn_gain[...]).astype(bf16)
        return _

    lax.fori_loop(0, length // high, norm_rows, 0)
    gather = RowGather(m, rows, row_send, row_recv)
    gather.start()
    for s in range(3, m.ring):
        for p in (0, 1):
            m.push(FFN, p, s)
        if s == 3:
            gather.forward()
    if m.ring < 4:
        gather.forward()
    for p in (0, 1):
        m.push(DOWN, p, 1)
    gather.finish()
    for k in range(4):
        gather.ready(k)
    m.arrived(FFN)

    def feed(i, _):
        at = pl.ds(2 * i, 2)
        block = rows[at].reshape(2 * length, width)
        both = jnp.dot(block, ffn_q[...], preferred_element_type=f32)
        block = (jax.nn.silu(both[:, :units]) * both[:, units:]).astype(bf16)
        hidden[0, i] = block[:length]
        hidden[1, i] = block[length:]
        return _

    lax.fori_loop(0, 4, feed, 0)
    m.push(DOWN, 0, 2)
    for phase in range(1, final + 1):
        t, first, count = phases[phase]
        if t == last_t:
            if first < size:
                m.ring_copy(DOWN, 0, t).wait_recv()
            if first >= size or count > size:
                for i in range(m.pieces) if count > size else ((first - size) // 128,):
                    m.piece_copy(i).wait_recv()
        elif t == 1:
            m.push(DOWN, 1, 2)
        elif t:
            for p in (0, 1):
                m.push(DOWN, p, t + 1)
        ffn_far_sums(phase)
        ffn_near_sums(phase)
        if phase > 1 and phase - 1 not in direct:
            forward_sums(phase - 1)
    count = final_count
    blocks = width // count
    final_block = (phase_base(final) * size + phases[direct[0]][1]) // count
    before_final = pl.ds(0, width - count)
    received(x_in.at[1, pl.ds(0, 2), :, before_final], x_last.at[1])

    def finish(block, parts):
        at = pl.ds(pl.multiple_of(block * count, count), count)
        done = middle[:, at].astype(f32) + total[1, :, at]
        for k in range(parts):
            done = done + x_in[1, k, :, at].astype(f32)
        finished[:, at] = done.astype(bf16)
        pltpu.make_async_copy(finished.at[:, at], result.at[:, at], end_sem).start()

    def finish_others(j, _):
        finish((final_block + j) % blocks, 2)
        return _

    lax.fori_loop(1, blocks, finish_others, 0)
    final_columns = pl.ds(pl.multiple_of(final_block * count, count), count)
    received(x_in.at[1, :, :, final_columns], x_last.at[2])
    finish(final_block, 3)
    gather.sent()
    for b in (0, 1):
        sums_sent(b)
    for w in (MODULE, OUT, FFN, DOWN):
        m.sent(w)
    pltpu.make_async_copy(finished, result, end_sem).wait()


def body(
    tokens,
    mix_gain,
    value_weight,
    gate_weight,
    conv_taps,
    head_gain,
    out_weight,
    ffn_gain,
    ffn_gate_weight,
    ffn_up_weight,
    down_weight,
):
    n_rep, n_fs, n_tp = lax.axis_size("rep"), lax.axis_size("fs"), lax.axis_size("tp")
    length, seq_count, width = tokens.shape
    assert n_rep == 2 and n_tp == 2 and n_fs % 2 == 0 and n_fs > 4 and seq_count == 1
    ring = n_fs // 2
    kernel = conv_taps.shape[0]
    channels, units = out_weight.shape[0] // 4, down_weight.shape[0] // 4
    pad = -(-(kernel // 2) // 8) * 8
    sem = pltpu.SemaphoreType.DMA
    operands = (
        tokens.reshape(length, width),
        mix_gain.reshape(1, width),
        value_weight,
        gate_weight,
        conv_taps,
        head_gain.reshape(1, -1),
        out_weight,
        ffn_gain.reshape(1, width),
        ffn_gate_weight,
        ffn_up_weight,
        down_weight,
    )
    layer_rows = pl.pallas_call(
        functools.partial(layer_kernel, n_rep, n_fs),
        out_shape=jax.ShapeDtypeStruct((length, width), bf16),
        in_specs=[pl.BlockSpec(memory_space=pl.ANY)] * len(operands),
        out_specs=pl.BlockSpec(memory_space=pl.ANY),
        scratch_shapes=[
            pltpu.VMEM((value_weight.shape[0], 8 * channels), bf16),
            pltpu.VMEM(out_weight.shape, bf16),
            pltpu.VMEM((ffn_gate_weight.shape[0], 8 * units), bf16),
            pltpu.VMEM(down_weight.shape, bf16),
            pltpu.VMEM((width, 2 * channels), bf16),
            pltpu.VMEM((n_fs, channels, out_weight.shape[1]), bf16),
            pltpu.VMEM((width, 2 * units), bf16),
            pltpu.VMEM((n_fs, units, down_weight.shape[1]), bf16),
            pltpu.VMEM((length, width), bf16),
            pltpu.VMEM((1, width), f32),
            pltpu.VMEM(conv_taps.shape, f32),
            pltpu.VMEM((1, head_gain.shape[0]), f32),
            pltpu.VMEM((1, width), f32),
            pltpu.VMEM((8, length, width), bf16),
            pltpu.VMEM((8, length, width), bf16),
            pltpu.VMEM((4, 2 * length + 2 * pad, channels), f32),
            pltpu.VMEM((4, 2 * length, channels), bf16),
            pltpu.VMEM((2, 4, length, units), bf16),
            pltpu.VMEM((length, width), bf16),
            pltpu.VMEM((2, length, width), f32),
            pltpu.VMEM((2, 4, length, width), bf16),
            pltpu.VMEM((2, 4, length, width), bf16),
            pltpu.VMEM((2, 3, length, width), bf16),
            pltpu.VMEM((2, 3, length, width), bf16),
            pltpu.VMEM((length, width), bf16),
        ]
        + [sem((4,)), sem((4, 2, ring - 1)), sem((max(1, down_weight.shape[1] // 128),)), sem((4,))]
        + [sem, sem((11,)), sem((2,)), sem((2, 2)), sem((2,)), sem((ring + 1 + down_weight.shape[1] // 128,))]
        + [sem((3,)), sem((4,)), sem((5,)), sem],
        compiler_params=pltpu.CompilerParams(
            collective_id=0, has_side_effects=True, vmem_limit_bytes=60 * 1024 * 1024
        ),
    )(*operands)
    return layer_rows.reshape(length, seq_count, width)


def solution(mesh):
    placed = (
        P("tp", ("rep", "fs"), None),
        P(),
        P("fs", "tp"),
        P("fs", "tp"),
        P(None, "tp"),
        P("tp"),
        P("tp", "fs"),
        P(),
        P("fs", "tp"),
        P("fs", "tp"),
        P("tp", "fs"),
    )
    return jax.shard_map(
        body, mesh=mesh, in_specs=placed, out_specs=P("tp", ("rep", "fs"), None), check_vma=False
    )
```

```python
import functools

import jax
import jax.numpy as jnp
from jax import lax
from jax.experimental import pallas as pl
from jax.experimental.pallas import tpu as pltpu
from jax.sharding import PartitionSpec as P

HEAD_DIM = 128
MESH = pl.DeviceIdType.MESH

norm_eps = 1e-06
group_eps = 1e-05
f32 = jnp.float32
bf16 = jnp.bfloat16


def rms_scale(matrix, scales):
    return matrix * lax.rsqrt(jnp.mean(matrix * matrix, axis=-1, keepdims=True) + norm_eps) * scales


MODULE, OUT, FFN, DOWN = range(4)


class Moves:
    def __init__(self, n_rep, n_fs, sources, wholes, axes, sems):
        self.rep, self.fs, self.tp = lax.axis_index("rep"), lax.axis_index("fs"), lax.axis_index("tp")
        rep, fs, tp = self.rep, self.fs, self.tp
        self.n_fs, self.line = n_fs, n_fs // 2
        self.pair, self.place = fs % 2, fs // 2
        flip = fs + 1 - 2 * self.pair
        self.to_tp = (rep, fs, 1 - tp)
        self.peers = (None, (rep, flip, tp), (1 - rep, fs, tp), (1 - rep, flip, tp))
        self.ends = ((rep, (fs + 2) % n_fs, tp), (rep, (fs + n_fs - 2) % n_fs, tp))
        self.has = (self.place < self.line - 1, self.place > 0)
        self.quarter = rep * 2 + self.pair
        self.other = rep * 2 + 1 - self.pair
        self.sources, self.wholes, self.axes = sources, wholes, axes
        self.send, self.line_recv, self.down_recv, self.pair_recv = sems
        self.pieces = max(1, wholes[DOWN].shape[2] // 128)

    def greet(self):
        def signal(device):
            pl.semaphore_signal(pltpu.get_barrier_semaphore(), inc=1, device_id=device, device_id_type=MESH)

        for side in (0, 1):
            pl.when(self.has[side])(functools.partial(signal, self.ends[side]))
        for device in self.peers[1:] + (self.to_tp,):
            signal(device)

    def meet(self):
        inside = jnp.logical_and(*self.has)

        @pl.when(inside)
        def _():
            pl.semaphore_wait(pltpu.get_barrier_semaphore(), 6)

        @pl.when(jnp.logical_not(inside))
        def _():
            pl.semaphore_wait(pltpu.get_barrier_semaphore(), 5)

    def part(self, w, quarter):
        size = self.sources[w].shape[self.axes[w]] // 4
        at = pl.ds(pl.multiple_of(quarter * size, size), size)
        return (slice(None), at) if self.axes[w] == 1 else (at, slice(None))

    def slots(self, w, owner, count=1):
        if self.axes[w] == 0:
            return (owner,) if count == 1 else (pl.ds(owner, count),)
        size = self.sources[w].shape[0]
        return (pl.ds(pl.multiple_of(owner * size, size), count * size), slice(None))

    def copy(self, src, dst, device, send_sem, recv_sem):
        return pltpu.make_async_remote_copy(
            src_ref=src,
            dst_ref=dst,
            send_sem=send_sem,
            recv_sem=recv_sem,
            device_id=device,
            device_id_type=MESH,
        )

    def pair_copy(self, w):
        source, there = self.sources[w].at[self.part(w, self.other)], self.wholes[w].at[self.slots(w, self.fs)]
        return self.copy(source, there, self.peers[1], self.send.at[w, 2], self.pair_recv.at[w])

    def line_copy(self, w, p, owner, side, own=False):
        if w == DOWN:
            there = self.wholes[w].at[owner * 2 + min(p, 1)]
            if p:
                columns = there.shape[1] // self.pieces
                there = there.at[:, pl.ds((p - 1) * columns, columns)]
            recv_sem = self.down_recv.at[p, owner]
        else:
            parity = self.pair if p == 0 else 1 - self.pair
            there = self.wholes[w].at[self.slots(w, owner * 2 + parity)]
            recv_sem = self.line_recv.at[w, p, owner]
        here = self.sources[w].at[self.part(w, self.quarter)] if own and w != DOWN and p == 0 else there
        return self.copy(here, there, self.ends[side], self.send.at[w, side], recv_sem)

    def push_own_ffn(self, lead):
        rows = self.sources[FFN].shape[0]
        at = pl.ds(0, rows // 4) if lead else pl.ds(rows // 4, rows - rows // 4)
        there = self.wholes[FFN].at[self.slots(FFN, self.fs)].at[at, :]
        here = self.sources[FFN].at[self.part(FFN, self.quarter)].at[at, :]
        for side in (0, 1):
            copy = self.copy(here, there, self.ends[side], self.send.at[FFN, side], self.line_recv.at[FFN, 0, self.place])
            pl.when(self.has[side])(copy.start)

    def push(self, w, p, s):
        if s == 1:
            if p == (0 if w == DOWN else 1):
                self.pair_copy(w).wait_recv()
            for side in (0, 1):
                pl.when(self.has[side])(self.line_copy(w, p, self.place, side, True).start)
            return
        for side in (0, 1):
            owner = self.place - (s - 1) if side == 0 else self.place + (s - 1)

            @pl.when((owner >= 0) if side == 0 else (owner < self.line))
            def _():
                copy = self.line_copy(w, p, owner, side)
                copy.wait_recv()
                pl.when(self.has[side])(copy.start)

    def arrived(self, w):
        for p in (0, 1):
            self.push(w, p, self.line)

    def nearest(self, t):
        left, right = self.place, self.line - 1 - self.place
        both = jnp.minimum(left, right)
        near = self.place - (t + 1) // 2 if t % 2 else self.place + t // 2
        far = jnp.where(right > left, self.place + (t - both), self.place - (t - both))
        return jnp.where(t <= 2 * both, near, far)

    def sent(self):
        for w in range(4):
            self.pair_copy(w).wait_send()
        for place in range(self.line):

            @pl.when(self.place == place)
            def _():
                for w in range(4):
                    for side, count in ((0, place + 1), (1, self.line - place)):
                        if count < self.line:
                            shards = self.wholes[w].at[self.slots(w, 0, 2 * count)]
                            self.copy(shards, shards, self.ends[side], self.send.at[w, side], self.pair_recv.at[w]).wait_send()


class RowGather:
    def __init__(self, m, rows, send_sem, recv_sems):
        half = rows.shape[1] // 2
        low, high = pl.ds(0, half), pl.ds(half, half)
        _, pair, rep, _ = m.peers
        first, near_pair, near_rep, across = (2 * k + m.tp for k in range(4))
        moves = (
            (rows.at[first, low], rows.at[near_rep, low], rep),
            (rows.at[first, high], rows.at[near_pair, high], pair),
            (rows.at[first, high], rows.at[near_rep, high], rep),
            (rows.at[first, low], rows.at[near_pair, low], pair),
            (rows.at[near_rep, low], rows.at[across, low], pair),
            (rows.at[near_pair, high], rows.at[across, high], rep),
            (rows.at[first], rows.at[first], m.to_tp),
            (rows.at[near_rep], rows.at[near_rep], m.to_tp),
            (rows.at[near_pair], rows.at[near_pair], m.to_tp),
            (rows.at[across, low], rows.at[across, low], m.to_tp),
            (rows.at[across, high], rows.at[across, high], m.to_tp),
        )
        self.copies = [m.copy(*move, send_sem, recv_sems.at[i]) for i, move in enumerate(moves)]
        seven = rows.at[pl.ds(0, 7)]
        self.all_sent = m.copy(seven, seven, pair, send_sem, recv_sems.at[0])

    def start(self):
        for i in (0, 1, 2, 3, 6):
            self.copies[i].start()

    def forward(self):
        for i in (0, 1):
            self.copies[i].wait_recv()
            self.copies[i + 4].start()

    def finish(self):
        for i in (2, 3, 4, 5):
            self.copies[i].wait_recv()
            self.copies[i + 5].start()

    def ready(self, k):
        for i in ((6,), (8,), (7,), (9, 10))[k]:
            self.copies[i].wait_recv()

    def sent(self):
        self.all_sent.wait_send()


def layer_kernel(
    n_rep, n_fs, tokens_in, mix_gain_in, value, gate, taps_in, head_gain_in, out, ffn_gain_in, ffn_gate, ffn_up,
    down, result,
    *scratch,
):
    staged, wholes, scratch = scratch[:4], scratch[4:8], scratch[8:]
    module_q, out_q, ffn_q, down_q = wholes
    tokens, mix_gain, taps, head_gain, ffn_gain = scratch[:5]
    rows_a, rows, padded, activated, hidden, middle, total, tp_out, tp_in, x_out, x_in, finished = scratch[5:17]
    weight_sems, scratch = scratch[17:21], scratch[21:]
    row_send, row_recv, tp_send, tp_recv, x_send, x_first, x_last, stage_sem, small_sem, end_sem = scratch
    channels, units = out_q.shape[1], down_q.shape[1]
    m = Moves(n_rep, n_fs, staged, wholes, (1, 0, 1, 0), weight_sems)
    length, width = tokens.shape
    kernel = taps.shape[0]
    pad = (padded.shape[1] - 2 * length) // 2
    tile = 512
    high = 32
    near_at = pl.ds(pl.multiple_of(m.tp * length, length), length)
    far_at = pl.ds(pl.multiple_of((1 - m.tp) * length, length), length)

    def stage(w, shards):
        if len(shards) == 1:
            pltpu.make_async_copy(shards[0], staged[w], stage_sem.at[w]).start()
            return
        size = shards[0].shape[1] // 4
        for i, shard in enumerate(shards):
            for q in range(4):
                there = staged[w].at[:, pl.ds((2 * q + i) * size, size)]
                pltpu.make_async_copy(shard.at[:, pl.ds(q * size, size)], there, stage_sem.at[w]).start()

    def stage_wait(w):
        pltpu.make_async_copy(staged[w], staged[w], stage_sem.at[w]).wait()

    def place(w, wait):
        there = wholes[w].at[m.slots(w, m.fs)]
        copy = pltpu.make_async_copy(staged[w].at[m.part(w, m.quarter)], there, stage_sem.at[w])
        copy.wait() if wait else copy.start()

    smalls = ((tokens_in, tokens), (mix_gain_in, mix_gain), (taps_in, taps))
    smalls += ((head_gain_in, head_gain), (ffn_gain_in, ffn_gain))
    small = [pltpu.make_async_copy(s, d, small_sem.at[i]) for i, (s, d) in enumerate(smalls)]
    m.greet()
    stage(MODULE, (value, gate))
    stage(OUT, (out,))
    small[0].start()
    small[1].start()
    stage(FFN, (ffn_gate, ffn_up))
    stage(DOWN, (down,))
    for copy in small[2:]:
        copy.start()
    stage_wait(MODULE)
    m.meet()
    m.pair_copy(MODULE).start()
    m.push(MODULE, 0, 1)
    stage_wait(OUT)
    m.pair_copy(OUT).start()
    m.push(OUT, 0, 1)
    stage_wait(FFN)
    m.push_own_ffn(True)

    def module_norm(i, _):
        at = pl.ds(pl.multiple_of(i * high, high), high)
        rows_a[m.tp, at, :] = rms_scale(tokens[at, :].astype(f32), mix_gain[...]).astype(bf16)
        return _

    small[0].wait()
    small[1].wait()
    lax.fori_loop(0, length // high, module_norm, 0)
    gather = RowGather(m, rows_a, row_send, row_recv)
    gather.start()
    m.push(MODULE, 1, 1)
    stage_wait(DOWN)
    for w in (MODULE, OUT, FFN, DOWN):
        place(w, False)
    zeros = jnp.zeros((4, pad, channels), f32)
    padded[:, pl.ds(0, pad), :] = zeros
    padded[:, pl.ds(pad + 2 * length, pad), :] = zeros
    for s in range(2, m.line):
        m.push(MODULE, 0, s)
        if s > 2:
            m.push(OUT, 0, s - 1)
        m.push(OUT, 1, s - 1)
        m.push(MODULE, 1, s)
        if s == 2:
            gather.forward()
            m.pair_copy(FFN).start()
    for p in (0, 1):
        m.push(OUT, p, m.line - 1)
    m.push_own_ffn(False)
    gather.finish()
    for w in (MODULE, OUT, FFN, DOWN):
        place(w, True)
    for copy in small[2:]:
        copy.wait()
    m.arrived(MODULE)

    def gated(k):
        block = rows_a[pl.ds(2 * k, 2)].reshape(2 * length, width)
        both = jnp.dot(block, module_q[...], preferred_element_type=f32)
        glu = (both[:, :channels] * jax.nn.sigmoid(both[:, channels:])).astype(bf16)
        padded[k, pl.ds(pad, 2 * length), :] = glu.astype(f32)

    channels_at = pl.ds(pl.multiple_of(m.quarter * channels, channels), channels)
    conv_rows = 64

    def convolve(k, _):
        for first in range(0, 2 * length, conv_rows):
            conved = jnp.zeros((conv_rows, channels), f32)
            for t in range(kernel):
                shifted = padded[k, pl.ds(first + t + pad - kernel // 2, conv_rows), :]
                conved = conved + shifted * taps[pl.ds(t, 1), channels_at]
            gains = head_gain[:, channels_at]
            for g in range(0, channels, HEAD_DIM):
                grouped = conved[:, g : g + HEAD_DIM]
                head_mean = jnp.mean(grouped, axis=-1, keepdims=True)
                head_var = jnp.mean(jnp.square(grouped - head_mean), axis=-1, keepdims=True)
                scaled = (grouped - head_mean) * lax.rsqrt(head_var + group_eps) * gains[:, g : g + HEAD_DIM]
                activated[k, pl.ds(first, conv_rows), pl.ds(g, HEAD_DIM)] = jax.nn.silu(scaled).astype(bf16)
        return _

    for k in range(4):
        gather.ready(k)
        gated(k)
    m.push(FFN, 1, 1)
    lax.fori_loop(0, 4, convolve, 0)
    m.arrived(OUT)

    def columns(weight, c):
        slots = tile // weight.shape[2]
        return jnp.concatenate([weight[c * slots + i] for i in range(slots)], axis=1)

    def tile_loop(step):
        def run(c, _):
            step(columns(out_q, c), pl.ds(pl.multiple_of(c * tile, tile), tile))
            return _

        lax.fori_loop(0, width // tile, run, 0)

    size = down_q.shape[2]
    last_t = m.line - 1
    phases = [None] + [(t, 0, 2 * size) for t in range(last_t)]
    if size % 128 == 0:
        phases += [(last_t, 0, size)] + [(last_t, size + c, 128) for c in range(0, size, 128)]
    else:
        phases += [(last_t, 0, 2 * size)]
    final = len(phases) - 1
    direct = [i for i in range(1, final + 1) if phases[i][0] == last_t and (phases[i][1] or i == final)]
    final_count = sum(phases[i][2] for i in direct)

    def phase_base(phase):
        return m.nearest(phases[phase][0]) * 2

    def phase_columns(phase):
        if phase == 0:
            return slice(None)
        _, first, count = phases[phase]
        return pl.ds(pl.multiple_of(phase_base(phase) * size + first, count), count)

    def phase_weight(phase):
        _, first, count = phases[phase]
        base = phase_base(phase)
        if count == 2 * size:
            return jnp.concatenate([down_q[base], down_q[base + 1]], axis=1)
        return down_q[base + first // size, :, pl.ds(first % size, count)]

    def tp_copy(phase, k, count=1):
        b, at = min(phase, 1), (pl.ds(k, count), slice(None), phase_columns(phase))
        recv_sem = tp_recv.at[phase % 2, 0 if k == 3 else 1]
        return m.copy(tp_out.at[(b, *at)], tp_in.at[(b, *at)], m.to_tp, tp_send.at[b], recv_sem)

    def x_copy(phase, k, low):
        b, columns_at = min(phase, 1), phase_columns(phase)
        at = pl.ds(0, length // 2) if low else pl.ds(length // 2, length // 2)
        to_rep = k == 2 or (k == 3 and low)
        there = (b, k - 1, at, columns_at)
        recv_sem = x_first.at[phase] if k == 3 else x_last.at[b]
        return m.copy(x_out.at[there], x_in.at[there], m.peers[2 if to_rep else 1], x_send.at[b], recv_sem)

    def direct_copy(phase, k):
        there = (1, k - 1, slice(None), phase_columns(phase))
        return m.copy(x_out.at[there], x_in.at[there], m.peers[k], x_send.at[1], x_last.at[2])

    def received(ref, sem):
        m.copy(ref, ref, m.peers[1], x_send.at[0], sem).wait_recv()

    def far_sums(k):
        def step(weight, at):
            product = jnp.dot(activated[k, far_at, :], weight, preferred_element_type=f32)
            tp_out[0, k, :, at] = product.astype(bf16)

        tile_loop(step)
        tp_copy(0, k).start()

    def near_sums(k):
        def step(weight, at):
            part = jnp.dot(activated[k, near_at, :], weight, preferred_element_type=f32)
            part = part + tp_in[0, k, :, at].astype(f32)
            if k == 0:
                total[0, :, at] = part
            else:
                x_out[0, k - 1, :, at] = part.astype(bf16)

        tile_loop(step)
        if k == 3:
            x_copy(0, 3, 1).start()
            x_copy(0, 3, 0).start()
        elif k:
            x_copy(0, k, k - 1).start()

    def ffn_far_sums(phase):
        _, _, count = phases[phase]
        product = jnp.dot(
            hidden[1 - m.tp].reshape(4 * length, units), phase_weight(phase), preferred_element_type=f32
        )
        tp_out[1, :, :, phase_columns(phase)] = product.astype(bf16).reshape(4, length, count)
        tp_copy(phase, 3).start()
        tp_copy(phase, 0, 3).start()

    def ffn_near_sums(phase):
        at = phase_columns(phase)
        parts = jnp.dot(hidden[m.tp].reshape(4 * length, units), phase_weight(phase), preferred_element_type=f32)
        tp_copy(phase, 3).wait_recv()
        for k in (3, 2, 1, 0):
            if k == 2:
                tp_copy(phase, 0, 3).wait_recv()
            part = parts[k * length : (k + 1) * length] + tp_in[1, k, :, at].astype(f32)
            if k == 0:
                total[1, :, at] = part
                continue
            x_out[1, k - 1, :, at] = part.astype(bf16)
            if phase in direct:
                direct_copy(phase, k).start()
            elif k == 3:
                x_copy(phase, 3, 1).start()
                x_copy(phase, 3, 0).start()
            else:
                x_copy(phase, k, k - 1).start()

    def forward_sums(phase):
        b, columns_at = min(phase, 1), phase_columns(phase)
        received(x_in.at[b, 2, :, columns_at], x_first.at[phase])
        for k, low in ((1, 1), (2, 0)):
            first = 0 if low else length // 2

            def add(i, _):
                at = pl.ds(pl.multiple_of(first + i * high, high), high)
                part = x_out[b, k - 1, at, columns_at].astype(f32)
                part = part + x_in[b, 2, at, columns_at].astype(f32)
                x_out[b, k - 1, at, columns_at] = part.astype(bf16)
                return _

            lax.fori_loop(0, length // (2 * high), add, 0)
            x_copy(phase, k, low).start()

    def sums_sent(b):
        m.copy(tp_out.at[b], tp_out.at[b], m.to_tp, tp_send.at[b], x_last.at[b]).wait_send()
        m.copy(x_out.at[b], x_out.at[b], m.peers[1], x_send.at[b], x_last.at[b]).wait_send()

    def all_sums(b, at):
        part = total[b, at, :]
        for k in (1, 2):
            part = part + x_in[b, k - 1, at, :].astype(f32)
        return part

    far_sums(3)
    far_sums(2)
    tp_copy(0, 3).wait_recv()
    near_sums(3)
    far_sums(1)
    far_sums(0)
    tp_copy(0, 0, 3).wait_recv()
    for k in (2, 1, 0):
        near_sums(k)
    m.push(FFN, 0, 2)
    forward_sums(0)
    m.push(FFN, 1, 2)
    m.pair_copy(DOWN).start()
    gather.sent()
    received(x_in.at[0, pl.ds(0, 2)], x_last.at[0])

    def norm_rows(i, _):
        at = pl.ds(pl.multiple_of(i * high, high), high)
        mid = (tokens[at, :].astype(f32) + all_sums(0, at)).astype(bf16)
        middle[at, :] = mid
        rows[m.tp, at, :] = rms_scale(mid.astype(f32), ffn_gain[...]).astype(bf16)
        return _

    lax.fori_loop(0, length // high, norm_rows, 0)
    gather = RowGather(m, rows, row_send, row_recv)
    gather.start()
    for s in range(3, m.line):
        for p in (0, 1):
            m.push(FFN, p, s)
        if s == 3:
            gather.forward()
    if m.line < 4:
        gather.forward()
    for p in range(1 + m.pieces):
        m.push(DOWN, p, 1)
    gather.finish()
    for k in range(4):
        gather.ready(k)
    m.arrived(FFN)

    def feed(i, _):
        at = pl.ds(2 * i, 2)
        block = rows[at].reshape(2 * length, width)
        both = jnp.dot(block, ffn_q[...], preferred_element_type=f32)
        block = (jax.nn.silu(both[:, :units]) * both[:, units:]).astype(bf16)
        hidden[0, i] = block[:length]
        hidden[1, i] = block[length:]
        return _

    lax.fori_loop(0, 4, feed, 0)
    m.push(DOWN, 0, 2)
    for phase in range(1, final + 1):
        t, first, count = phases[phase]
        for p in range(1 + m.pieces):
            begin = p if p == 0 else size + (p - 1) * size // m.pieces
            if t and (t, p) != (1, 0) and (t < last_t or first <= begin < first + count):
                m.push(DOWN, p, t + 1)
        ffn_far_sums(phase)
        ffn_near_sums(phase)
        if phase > 1 and phase - 1 not in direct:
            forward_sums(phase - 1)
    count = final_count
    blocks = width // count
    final_block = (phase_base(final) * size + phases[direct[0]][1]) // count
    before_final = pl.ds(0, width - count)
    received(x_in.at[1, pl.ds(0, 2), :, before_final], x_last.at[1])

    def finish(block, parts):
        at = pl.ds(pl.multiple_of(block * count, count), count)
        done = middle[:, at].astype(f32) + total[1, :, at]
        for k in range(parts):
            done = done + x_in[1, k, :, at].astype(f32)
        finished[:, at] = done.astype(bf16)
        pltpu.make_async_copy(finished.at[:, at], result.at[:, at], end_sem).start()

    def finish_others(j, _):
        finish((final_block + j) % blocks, 2)
        return _

    lax.fori_loop(1, blocks, finish_others, 0)
    final_columns = pl.ds(pl.multiple_of(final_block * count, count), count)
    received(x_in.at[1, :, :, final_columns], x_last.at[2])
    finish(final_block, 3)
    gather.sent()
    for b in (0, 1):
        sums_sent(b)
    m.sent()
    pltpu.make_async_copy(finished, result, end_sem).wait()


def body(
    tokens,
    mix_gain,
    value_weight,
    gate_weight,
    conv_taps,
    head_gain,
    out_weight,
    ffn_gain,
    ffn_gate_weight,
    ffn_up_weight,
    down_weight,
):
    n_rep, n_fs, n_tp = lax.axis_size("rep"), lax.axis_size("fs"), lax.axis_size("tp")
    length, seq_count, width = tokens.shape
    assert n_rep == 2 and n_tp == 2 and n_fs % 2 == 0 and n_fs > 4 and seq_count == 1
    line = n_fs // 2
    kernel = conv_taps.shape[0]
    channels, units = out_weight.shape[0] // 4, down_weight.shape[0] // 4
    pad = -(-(kernel // 2) // 8) * 8
    sem = pltpu.SemaphoreType.DMA
    operands = (
        tokens.reshape(length, width),
        mix_gain.reshape(1, width),
        value_weight,
        gate_weight,
        conv_taps,
        head_gain.reshape(1, -1),
        out_weight,
        ffn_gain.reshape(1, width),
        ffn_gate_weight,
        ffn_up_weight,
        down_weight,
    )
    layer_rows = pl.pallas_call(
        functools.partial(layer_kernel, n_rep, n_fs),
        out_shape=jax.ShapeDtypeStruct((length, width), bf16),
        in_specs=[pl.BlockSpec(memory_space=pl.ANY)] * len(operands),
        out_specs=pl.BlockSpec(memory_space=pl.ANY),
        scratch_shapes=[
            pltpu.VMEM((value_weight.shape[0], 8 * channels), bf16),
            pltpu.VMEM(out_weight.shape, bf16),
            pltpu.VMEM((ffn_gate_weight.shape[0], 8 * units), bf16),
            pltpu.VMEM(down_weight.shape, bf16),
            pltpu.VMEM((width, 2 * channels), bf16),
            pltpu.VMEM((n_fs, channels, out_weight.shape[1]), bf16),
            pltpu.VMEM((width, 2 * units), bf16),
            pltpu.VMEM((n_fs, units, down_weight.shape[1]), bf16),
            pltpu.VMEM((length, width), bf16),
            pltpu.VMEM((1, width), f32),
            pltpu.VMEM(conv_taps.shape, f32),
            pltpu.VMEM((1, head_gain.shape[0]), f32),
            pltpu.VMEM((1, width), f32),
            pltpu.VMEM((8, length, width), bf16),
            pltpu.VMEM((8, length, width), bf16),
            pltpu.VMEM((4, 2 * length + 2 * pad, channels), f32),
            pltpu.VMEM((4, 2 * length, channels), bf16),
            pltpu.VMEM((2, 4, length, units), bf16),
            pltpu.VMEM((length, width), bf16),
            pltpu.VMEM((2, length, width), f32),
            pltpu.VMEM((2, 4, length, width), bf16),
            pltpu.VMEM((2, 4, length, width), bf16),
            pltpu.VMEM((2, 3, length, width), bf16),
            pltpu.VMEM((2, 3, length, width), bf16),
            pltpu.VMEM((length, width), bf16),
        ]
        + [sem((4, 3)), sem((3, 2, line)), sem((1 + max(1, down_weight.shape[1] // 128), line)), sem((4,))]
        + [sem, sem((11,)), sem((2,)), sem((2, 2)), sem((2,)), sem((line + 1 + down_weight.shape[1] // 128,))]
        + [sem((3,)), sem((4,)), sem((5,)), sem],
        compiler_params=pltpu.CompilerParams(
            collective_id=0, has_side_effects=True, vmem_limit_bytes=60 * 1024 * 1024
        ),
    )(*operands)
    return layer_rows.reshape(length, seq_count, width)


def solution(mesh):
    placed = (
        P("tp", ("rep", "fs"), None),
        P(),
        P("fs", "tp"),
        P("fs", "tp"),
        P(None, "tp"),
        P("tp"),
        P("tp", "fs"),
        P(),
        P("fs", "tp"),
        P("fs", "tp"),
        P("tp", "fs"),
    )
    return jax.shard_map(
        body, mesh=mesh, in_specs=placed, out_specs=P("tp", ("rep", "fs"), None), check_vma=False
    )
```

```python
import functools

import jax
import jax.numpy as jnp
from jax import lax
from jax.experimental import pallas as pl
from jax.experimental.pallas import tpu as pltpu
from jax.sharding import PartitionSpec as P

HEAD_DIM = 128
MESH = pl.DeviceIdType.MESH

norm_eps = 1e-06
group_eps = 1e-05
f32 = jnp.float32
bf16 = jnp.bfloat16


def rms_scale(matrix, scales):
    return matrix * lax.rsqrt(jnp.mean(matrix * matrix, axis=-1, keepdims=True) + norm_eps) * scales


MODULE, OUT, FFN, DOWN = range(4)


def nearest(place, line, t):
    left, right = place, line - 1 - place
    both = jnp.minimum(left, right)
    near = place - (t + 1) // 2 if t % 2 else place + t // 2
    far = jnp.where(right > left, place + (t - both), place - (t - both))
    return jnp.where(t <= 2 * both, near, far)


def final_columns(place, line, size):
    count = size if size % 128 == 0 else 2 * size
    block = (nearest(place, line, line - 1) * 2 * size + 2 * size - count) // count
    return block, count


class Moves:
    def __init__(self, n_rep, n_fs, sources, wholes, axes, sems):
        self.rep, self.fs, self.tp = lax.axis_index("rep"), lax.axis_index("fs"), lax.axis_index("tp")
        rep, fs, tp = self.rep, self.fs, self.tp
        self.n_fs, self.line = n_fs, n_fs // 2
        self.pair, self.place = fs % 2, fs // 2
        flip = fs + 1 - 2 * self.pair
        self.to_tp = (rep, fs, 1 - tp)
        self.peers = (None, (rep, flip, tp), (1 - rep, fs, tp), (1 - rep, flip, tp))
        self.ends = ((rep, (fs + 2) % n_fs, tp), (rep, (fs + n_fs - 2) % n_fs, tp))
        self.has = (self.place < self.line - 1, self.place > 0)
        self.quarter = rep * 2 + self.pair
        self.other = rep * 2 + 1 - self.pair
        self.sources, self.wholes, self.axes = sources, wholes, axes
        self.send, self.line_recv, self.down_recv, self.pair_recv = sems
        self.pieces = max(1, wholes[DOWN].shape[2] // 128)

    def greet(self):
        def signal(device):
            pl.semaphore_signal(pltpu.get_barrier_semaphore(), inc=1, device_id=device, device_id_type=MESH)

        for side in (0, 1):
            pl.when(self.has[side])(functools.partial(signal, self.ends[side]))
        for device in self.peers[1:] + (self.to_tp,):
            signal(device)

    def meet(self):
        inside = jnp.logical_and(*self.has)

        @pl.when(inside)
        def _():
            pl.semaphore_wait(pltpu.get_barrier_semaphore(), 6)

        @pl.when(jnp.logical_not(inside))
        def _():
            pl.semaphore_wait(pltpu.get_barrier_semaphore(), 5)

    def part(self, w, quarter):
        size = self.sources[w].shape[self.axes[w]] // 4
        at = pl.ds(pl.multiple_of(quarter * size, size), size)
        return (slice(None), at) if self.axes[w] == 1 else (at, slice(None))

    def slots(self, w, owner, count=1):
        if self.axes[w] == 0:
            return (owner,) if count == 1 else (pl.ds(owner, count),)
        size = self.sources[w].shape[0]
        return (pl.ds(pl.multiple_of(owner * size, size), count * size), slice(None))

    def copy(self, src, dst, device, send_sem, recv_sem):
        return pltpu.make_async_remote_copy(
            src_ref=src,
            dst_ref=dst,
            send_sem=send_sem,
            recv_sem=recv_sem,
            device_id=device,
            device_id_type=MESH,
        )

    def pair_copy(self, w):
        source, there = self.sources[w].at[self.part(w, self.other)], self.wholes[w].at[self.slots(w, self.fs)]
        return self.copy(source, there, self.peers[1], self.send.at[w, 0], self.pair_recv.at[w])

    def line_copy(self, w, p, owner, side, own=False):
        if w == DOWN:
            there = self.wholes[w].at[owner * 2 + min(p, 1)]
            if p:
                columns = there.shape[1] // self.pieces
                there = there.at[:, pl.ds((p - 1) * columns, columns)]
            recv_sem = self.down_recv.at[p, owner - side]
        else:
            parity = self.pair if p == 0 else 1 - self.pair
            there = self.wholes[w].at[self.slots(w, owner * 2 + parity)]
            recv_sem = self.line_recv.at[w, p, owner - side]
        here = self.sources[w].at[self.part(w, self.quarter)] if own and w != DOWN and p == 0 else there
        return self.copy(here, there, self.ends[side], self.send.at[w, side], recv_sem)

    def push_own_ffn(self, lead):
        rows = self.sources[FFN].shape[0]
        at = pl.ds(0, rows // 4) if lead else pl.ds(rows // 4, rows - rows // 4)
        there = self.wholes[FFN].at[self.slots(FFN, self.fs)].at[at, :]
        here = self.sources[FFN].at[self.part(FFN, self.quarter)].at[at, :]
        for side in (0, 1):


            @pl.when(self.has[side])
            def _():
                recv_sem = self.line_recv.at[FFN, 0, self.place - side]
                self.copy(here, there, self.ends[side], self.send.at[FFN, side], recv_sem).start()

    def push(self, w, p, s):
        if s == 1:
            if p == (0 if w == DOWN else 1):
                self.pair_copy(w).wait_recv()
            for side in (0, 1):


                @pl.when(self.has[side])
                def _():
                    self.line_copy(w, p, self.place, side, True).start()

            return
        for side in (0, 1):
            owner = self.place - (s - 1) if side == 0 else self.place + (s - 1)

            @pl.when((owner >= 0) if side == 0 else (owner < self.line))
            def _():
                copy = self.line_copy(w, p, owner, side)
                copy.wait_recv()
                pl.when(self.has[side])(copy.start)

    def arrived(self, w):
        for p in (0, 1):
            self.push(w, p, self.line)

    def sent(self):
        for place in range(self.line):

            @pl.when(self.place == place)
            def _():
                for w in range(4):
                    for side, count in ((0, place + 1), (1, self.line - place)):
                        count = (2 * count if count < self.line else 0) + 1 - side
                        if count:
                            shards = self.wholes[w].at[self.slots(w, 0, count)]
                            self.copy(shards, shards, self.peers[1], self.send.at[w, side], self.pair_recv.at[w]).wait_send()


class RowGather:
    def __init__(self, m, rows, send_sem, recv_sems):
        half = rows.shape[1] // 2
        low, high = pl.ds(0, half), pl.ds(half, half)
        _, pair, rep, _ = m.peers
        first, near_pair, near_rep, across = (2 * k + m.tp for k in range(4))
        moves = (
            (rows.at[first, low], rows.at[near_rep, low], rep),
            (rows.at[first, high], rows.at[near_pair, high], pair),
            (rows.at[first, high], rows.at[near_rep, high], rep),
            (rows.at[first, low], rows.at[near_pair, low], pair),
            (rows.at[near_rep, low], rows.at[across, low], pair),
            (rows.at[near_pair, high], rows.at[across, high], rep),
            (rows.at[first], rows.at[first], m.to_tp),
            (rows.at[near_rep], rows.at[near_rep], m.to_tp),
            (rows.at[near_pair], rows.at[near_pair], m.to_tp),
            (rows.at[across], rows.at[across], m.to_tp),
        )
        self.copies = [m.copy(*move, send_sem, recv_sems.at[4 if i == 5 else i]) for i, move in enumerate(moves)]
        self.diagonal = m.copy(rows.at[across], rows.at[across], pair, send_sem, recv_sems.at[4])
        seven = rows.at[pl.ds(0, 7)]
        self.all_sent = m.copy(seven, seven, pair, send_sem, recv_sems.at[0])

    def start(self):
        for i in (0, 1, 2, 3, 6):
            self.copies[i].start()

    def forward(self):
        for i in (0, 1):
            self.copies[i].wait_recv()
            self.copies[i + 4].start()

    def finish(self):
        for i in (2, 3):
            self.copies[i].wait_recv()
            self.copies[i + 5].start()
        self.diagonal.wait_recv()
        self.copies[9].start()

    def ready(self, k):
        for i in ((6,), (8,), (7,), (9,))[k]:
            self.copies[i].wait_recv()

    def sent(self):
        self.all_sent.wait_send()


def layer_kernel(
    n_rep, n_fs, tokens_in, mix_gain_in, value, gate, taps_in, head_gain_in, out, ffn_gain_in, ffn_gate, ffn_up,
    down, early, partial, late,
    *scratch,
):
    staged, wholes, scratch = scratch[:4], scratch[4:8], scratch[8:]
    module_q, out_q, ffn_q, down_q = wholes
    tokens, mix_gain, taps, head_gain, ffn_gain = scratch[:5]
    rows_a, rows, padded, activated, hidden, middle, total, tp_out, tp_in, x_out, x_in, finished, last_partial = scratch[5:18]
    weight_sems, scratch = scratch[18:22], scratch[22:]
    row_send, row_recv, tp_send, tp_recv, x_send, x_first, x_last, stage_sem, small_sem, end_sem = scratch
    channels, units = out_q.shape[1], down_q.shape[1]
    m = Moves(n_rep, n_fs, staged, wholes, (1, 0, 1, 0), weight_sems)
    length, width = tokens.shape
    kernel = taps.shape[0]
    pad = (padded.shape[1] - 2 * length) // 2
    tile = 512
    high = 32
    near_at = pl.ds(pl.multiple_of(m.tp * length, length), length)
    far_at = pl.ds(pl.multiple_of((1 - m.tp) * length, length), length)

    def stage(w, shards):
        if len(shards) == 1:
            pltpu.make_async_copy(shards[0], staged[w], stage_sem.at[w]).start()
            return
        size = shards[0].shape[1] // 4
        for i, shard in enumerate(shards):
            for q in range(4):
                there = staged[w].at[:, pl.ds((2 * q + i) * size, size)]
                pltpu.make_async_copy(shard.at[:, pl.ds(q * size, size)], there, stage_sem.at[w]).start()

    def stage_wait(w):
        pltpu.make_async_copy(staged[w], staged[w], stage_sem.at[w]).wait()

    def place(w, wait):
        there = wholes[w].at[m.slots(w, m.fs)]
        copy = pltpu.make_async_copy(staged[w].at[m.part(w, m.quarter)], there, stage_sem.at[w])
        copy.wait() if wait else copy.start()

    smalls = ((tokens_in, tokens), (mix_gain_in, mix_gain), (taps_in, taps))
    smalls += ((head_gain_in, head_gain), (ffn_gain_in, ffn_gain))
    small = [pltpu.make_async_copy(s, d, small_sem.at[i]) for i, (s, d) in enumerate(smalls)]
    m.greet()
    stage(MODULE, (value, gate))
    stage(OUT, (out,))
    small[0].start()
    small[1].start()
    stage(FFN, (ffn_gate, ffn_up))
    stage(DOWN, (down,))
    for copy in small[2:]:
        copy.start()
    stage_wait(MODULE)
    m.meet()
    m.pair_copy(MODULE).start()
    m.push(MODULE, 0, 1)
    stage_wait(OUT)
    m.pair_copy(OUT).start()
    m.push(OUT, 0, 1)
    stage_wait(FFN)
    m.push_own_ffn(True)

    def module_norm(i, _):
        at = pl.ds(pl.multiple_of(i * high, high), high)
        rows_a[m.tp, at, :] = rms_scale(tokens[at, :].astype(f32), mix_gain[...]).astype(bf16)
        return _

    small[0].wait()
    small[1].wait()
    lax.fori_loop(0, length // high, module_norm, 0)
    gather = RowGather(m, rows_a, row_send, row_recv)
    gather.start()
    m.push(MODULE, 1, 1)
    stage_wait(DOWN)
    for w in (MODULE, OUT, FFN, DOWN):
        place(w, False)
    zeros = jnp.zeros((4, pad, channels), f32)
    padded[:, pl.ds(0, pad), :] = zeros
    padded[:, pl.ds(pad + 2 * length, pad), :] = zeros
    for s in range(2, m.line):
        m.push(MODULE, 0, s)
        if s > 2:
            m.push(OUT, 0, s - 1)
        m.push(OUT, 1, s - 1)
        m.push(MODULE, 1, s)
        if s == 2:
            gather.forward()
            m.pair_copy(FFN).start()
    for p in (0, 1):
        m.push(OUT, p, m.line - 1)
    m.push_own_ffn(False)
    gather.finish()
    for w in (MODULE, OUT, FFN, DOWN):
        place(w, True)
    for copy in small[2:]:
        copy.wait()
    m.arrived(MODULE)

    def gated(k):
        block = rows_a[pl.ds(2 * k, 2)].reshape(2 * length, width)
        both = jnp.dot(block, module_q[...], preferred_element_type=f32)
        glu = (both[:, :channels] * jax.nn.sigmoid(both[:, channels:])).astype(bf16)
        padded[k, pl.ds(pad, 2 * length), :] = glu.astype(f32)

    channels_at = pl.ds(pl.multiple_of(m.quarter * channels, channels), channels)
    conv_rows = 64

    def convolve(k, _):
        for first in range(0, 2 * length, conv_rows):
            conved = jnp.zeros((conv_rows, channels), f32)
            for t in range(kernel):
                shifted = padded[k, pl.ds(first + t + pad - kernel // 2, conv_rows), :]
                conved = conved + shifted * taps[pl.ds(t, 1), channels_at]
            gains = head_gain[:, channels_at]
            for g in range(0, channels, HEAD_DIM):
                grouped = conved[:, g : g + HEAD_DIM]
                head_mean = jnp.mean(grouped, axis=-1, keepdims=True)
                head_var = jnp.mean(jnp.square(grouped - head_mean), axis=-1, keepdims=True)
                scaled = (grouped - head_mean) * lax.rsqrt(head_var + group_eps) * gains[:, g : g + HEAD_DIM]
                activated[k, pl.ds(first, conv_rows), pl.ds(g, HEAD_DIM)] = jax.nn.silu(scaled).astype(bf16)
        return _

    for k in range(4):
        gather.ready(k)
        gated(k)
    m.push(FFN, 1, 1)
    lax.fori_loop(0, 4, convolve, 0)
    m.arrived(OUT)

    def columns(weight, c):
        slots = tile // weight.shape[2]
        return jnp.concatenate([weight[c * slots + i] for i in range(slots)], axis=1)

    def tile_loop(step):
        def run(c, _):
            step(columns(out_q, c), pl.ds(pl.multiple_of(c * tile, tile), tile))
            return _

        lax.fori_loop(0, width // tile, run, 0)

    size = down_q.shape[2]
    last_t = m.line - 1
    phases = [None] + [(t, 0, 2 * size) for t in range(last_t)]
    if size % 128 == 0:
        phases += [(last_t, 0, size)] + [(last_t, size + c, 128) for c in range(0, size, 128)]
    else:
        phases += [(last_t, 0, 2 * size)]
    final = len(phases) - 1
    direct = [i for i in range(1, final + 1) if phases[i][0] == last_t and (phases[i][1] or i == final)]

    def phase_base(phase):
        return nearest(m.place, m.line, phases[phase][0]) * 2

    def phase_columns(phase):
        if phase == 0:
            return slice(None)
        _, first, count = phases[phase]
        return pl.ds(pl.multiple_of(phase_base(phase) * size + first, count), count)

    def phase_weight(phase):
        _, first, count = phases[phase]
        base = phase_base(phase)
        if count == 2 * size:
            return jnp.concatenate([down_q[base], down_q[base + 1]], axis=1)
        return down_q[base + first // size, :, pl.ds(first % size, count)]

    def tp_copy(phase, k, count=1):
        b, at = min(phase, 1), (pl.ds(k, count), slice(None), phase_columns(phase))
        recv_sem = tp_recv.at[phase % 2, 0 if k == 3 else 1]
        return m.copy(tp_out.at[(b, *at)], tp_in.at[(b, *at)], m.to_tp, tp_send.at[b], recv_sem)

    def x_copy(phase, k, low):
        b, columns_at = min(phase, 1), phase_columns(phase)
        at = pl.ds(0, length // 2) if low else pl.ds(length // 2, length // 2)
        to_rep = k == 2 or (k == 3 and low)
        there = (b, k - 1, at, columns_at)
        recv_sem = x_first.at[phase] if k == 3 else x_last.at[b]
        return m.copy(x_out.at[there], x_in.at[there], m.peers[2 if to_rep else 1], x_send.at[b], recv_sem)

    def direct_copy(phase, k):
        source = x_out.at[1, k - 1, :, phase_columns(phase)]
        first, count = phases[phase][1] - phases[direct[0]][1], phases[phase][2]
        return m.copy(source, late.at[k - 1, :, pl.ds(first, count)], m.peers[k], x_send.at[1], x_last.at[2])

    def received(ref, sem):
        m.copy(ref, ref, m.peers[1], x_send.at[0], sem).wait_recv()

    def far_sums(k):
        def step(weight, at):
            product = jnp.dot(activated[k, far_at, :], weight, preferred_element_type=f32)
            tp_out[0, k, :, at] = product.astype(bf16)

        tile_loop(step)
        tp_copy(0, k).start()

    def near_sums(k):
        def step(weight, at):
            part = jnp.dot(activated[k, near_at, :], weight, preferred_element_type=f32)
            part = part + tp_in[0, k, :, at].astype(f32)
            if k == 0:
                total[0, :, at] = part
            else:
                x_out[0, k - 1, :, at] = part.astype(bf16)

        tile_loop(step)
        if k == 3:
            x_copy(0, 3, 1).start()
            x_copy(0, 3, 0).start()
        elif k:
            x_copy(0, k, k - 1).start()

    def ffn_far_sums(phase):
        _, _, count = phases[phase]
        product = jnp.dot(
            hidden[1 - m.tp].reshape(4 * length, units), phase_weight(phase), preferred_element_type=f32
        )
        tp_out[1, :, :, phase_columns(phase)] = product.astype(bf16).reshape(4, length, count)
        tp_copy(phase, 3).start()
        tp_copy(phase, 0, 3).start()

    def ffn_near_sums(phase):
        at = phase_columns(phase)
        parts = jnp.dot(hidden[m.tp].reshape(4 * length, units), phase_weight(phase), preferred_element_type=f32)
        tp_copy(phase, 3).wait_recv()
        for k in (3, 2, 1, 0):
            if k == 2:
                tp_copy(phase, 0, 3).wait_recv()
            part = parts[k * length : (k + 1) * length] + tp_in[1, k, :, at].astype(f32)
            if k == 0:
                total[1, :, at] = part
                continue
            x_out[1, k - 1, :, at] = part.astype(bf16)
            if phase in direct:
                direct_copy(phase, k).start()
            elif k == 3:
                x_copy(phase, 3, 1).start()
                x_copy(phase, 3, 0).start()
            else:
                x_copy(phase, k, k - 1).start()

    def forward_sums(phase):
        b, columns_at = min(phase, 1), phase_columns(phase)
        received(x_in.at[b, 2, :, columns_at], x_first.at[phase])
        for k, low in ((1, 1), (2, 0)):
            first = 0 if low else length // 2

            def add(i, _):
                at = pl.ds(pl.multiple_of(first + i * high, high), high)
                part = x_out[b, k - 1, at, columns_at].astype(f32)
                part = part + x_in[b, 2, at, columns_at].astype(f32)
                x_out[b, k - 1, at, columns_at] = part.astype(bf16)
                return _

            lax.fori_loop(0, length // (2 * high), add, 0)
            x_copy(phase, k, low).start()

    def sums_sent(b):
        m.copy(tp_out.at[b], tp_out.at[b], m.to_tp, tp_send.at[b], x_last.at[b]).wait_send()
        m.copy(x_out.at[b], x_out.at[b], m.peers[1], x_send.at[b], x_last.at[b]).wait_send()

    def all_sums(b, at):
        part = total[b, at, :]
        for k in (1, 2):
            part = part + x_in[b, k - 1, at, :].astype(f32)
        return part

    far_sums(3)
    far_sums(2)
    tp_copy(0, 3).wait_recv()
    near_sums(3)
    far_sums(1)
    far_sums(0)
    tp_copy(0, 0, 3).wait_recv()
    for k in (2, 1, 0):
        near_sums(k)
    m.push(FFN, 0, 2)
    forward_sums(0)
    m.push(FFN, 1, 2)
    m.pair_copy(DOWN).start()
    gather.sent()
    received(x_in.at[0, pl.ds(0, 2)], x_last.at[0])

    def norm_rows(i, _):
        at = pl.ds(pl.multiple_of(i * high, high), high)
        mid = (tokens[at, :].astype(f32) + all_sums(0, at)).astype(bf16)
        middle[at, :] = mid
        rows[m.tp, at, :] = rms_scale(mid.astype(f32), ffn_gain[...]).astype(bf16)
        return _

    lax.fori_loop(0, length // high, norm_rows, 0)
    gather = RowGather(m, rows, row_send, row_recv)
    gather.start()
    for s in range(3, m.line):
        for p in (0, 1):
            m.push(FFN, p, s)
        if s == 3:
            gather.forward()
    if m.line < 4:
        gather.forward()
    for p in range(1 + m.pieces):
        m.push(DOWN, p, 1)
    gather.finish()
    for k in range(4):
        gather.ready(k)
    m.arrived(FFN)

    def feed(i, _):
        at = pl.ds(2 * i, 2)
        block = rows[at].reshape(2 * length, width)
        both = jnp.dot(block, ffn_q[...], preferred_element_type=f32)
        block = (jax.nn.silu(both[:, :units]) * both[:, units:]).astype(bf16)
        hidden[0, i] = block[:length]
        hidden[1, i] = block[length:]
        return _

    lax.fori_loop(0, 4, feed, 0)
    m.push(DOWN, 0, 2)
    for phase in range(1, final + 1):
        t, first, count = phases[phase]
        for p in range(1 + m.pieces):
            begin = p if p == 0 else size + (p - 1) * size // m.pieces
            if t and (t, p) != (1, 0) and (t < last_t or first <= begin < first + count):
                m.push(DOWN, p, t + 1)
        ffn_far_sums(phase)
        ffn_near_sums(phase)
        if phase > 1 and phase - 1 not in direct:
            forward_sums(phase - 1)
    final_block, count = final_columns(m.place, m.line, size)
    final_at = pl.ds(pl.multiple_of(final_block * count, count), count)
    last_partial[...] = middle[:, final_at].astype(f32) + total[1, :, final_at]
    keep = pltpu.make_async_copy(last_partial, partial, end_sem.at[0])
    keep.start()
    blocks = width // count
    before_final = pl.ds(0, width - count)
    received(x_in.at[1, pl.ds(0, 2), :, before_final], x_last.at[1])

    def finish(j, _):
        block = (final_block + j) % blocks
        at = pl.ds(pl.multiple_of(block * count, count), count)
        done = middle[:, at].astype(f32) + total[1, :, at]
        for k in range(2):
            done = done + x_in[1, k, :, at].astype(f32)
        finished[:, at] = done.astype(bf16)
        pltpu.make_async_copy(finished.at[:, at], early.at[:, at], end_sem.at[1]).start()
        return _

    lax.fori_loop(1, blocks, finish, 0)
    gather.sent()
    sums_sent(0)
    m.sent()
    others = finished.at[:, before_final]
    pltpu.make_async_copy(others, others, end_sem.at[1]).wait()
    keep.wait()
    sums_sent(1)
    received(late, x_last.at[2])


def closing_kernel(n_fs, size, early, partial, late, result, rows, last, parts, sems):
    block, count = final_columns(lax.axis_index("fs") // 2, n_fs // 2, size)
    copies = [
        pltpu.make_async_copy(source, there, sems.at[i])
        for i, (source, there) in enumerate(((early, rows), (partial, last), (late, parts)))
    ]
    for copy in copies:
        copy.start()
    for copy in copies:
        copy.wait()
    done = last[...]
    for k in range(3):
        done = done + parts[k].astype(f32)
    rows[:, pl.ds(pl.multiple_of(block * count, count), count)] = done.astype(bf16)
    leave = pltpu.make_async_copy(rows, result, sems.at[3])
    leave.start()
    leave.wait()


def body(
    tokens,
    mix_gain,
    value_weight,
    gate_weight,
    conv_taps,
    head_gain,
    out_weight,
    ffn_gain,
    ffn_gate_weight,
    ffn_up_weight,
    down_weight,
):
    n_rep, n_fs, n_tp = lax.axis_size("rep"), lax.axis_size("fs"), lax.axis_size("tp")
    length, seq_count, width = tokens.shape
    assert n_rep == 2 and n_tp == 2 and n_fs % 2 == 0 and n_fs > 4 and seq_count == 1
    line = n_fs // 2
    kernel = conv_taps.shape[0]
    channels, units = out_weight.shape[0] // 4, down_weight.shape[0] // 4
    pad = -(-(kernel // 2) // 8) * 8
    sem = pltpu.SemaphoreType.DMA
    operands = (
        tokens.reshape(length, width),
        mix_gain.reshape(1, width),
        value_weight,
        gate_weight,
        conv_taps,
        head_gain.reshape(1, -1),
        out_weight,
        ffn_gain.reshape(1, width),
        ffn_gate_weight,
        ffn_up_weight,
        down_weight,
    )
    size = down_weight.shape[1]
    count = size if size % 128 == 0 else 2 * size
    late_shapes = (((length, width), bf16), ((length, count), f32), ((3, length, count), bf16))
    parts = pl.pallas_call(
        functools.partial(layer_kernel, n_rep, n_fs),
        out_shape=[jax.ShapeDtypeStruct(*shape) for shape in late_shapes],
        in_specs=[pl.BlockSpec(memory_space=pl.ANY)] * len(operands),
        out_specs=[pl.BlockSpec(memory_space=pl.ANY)] * 3,
        scratch_shapes=[
            pltpu.VMEM((value_weight.shape[0], 8 * channels), bf16),
            pltpu.VMEM(out_weight.shape, bf16),
            pltpu.VMEM((ffn_gate_weight.shape[0], 8 * units), bf16),
            pltpu.VMEM(down_weight.shape, bf16),
            pltpu.VMEM((width, 2 * channels), bf16),
            pltpu.VMEM((n_fs, channels, out_weight.shape[1]), bf16),
            pltpu.VMEM((width, 2 * units), bf16),
            pltpu.VMEM((n_fs, units, down_weight.shape[1]), bf16),
            pltpu.VMEM((length, width), bf16),
            pltpu.VMEM((1, width), f32),
            pltpu.VMEM(conv_taps.shape, f32),
            pltpu.VMEM((1, head_gain.shape[0]), f32),
            pltpu.VMEM((1, width), f32),
            pltpu.VMEM((8, length, width), bf16),
            pltpu.VMEM((8, length, width), bf16),
            pltpu.VMEM((4, 2 * length + 2 * pad, channels), f32),
            pltpu.VMEM((4, 2 * length, channels), bf16),
            pltpu.VMEM((2, 4, length, units), bf16),
            pltpu.VMEM((length, width), bf16),
            pltpu.VMEM((2, length, width), f32),
            pltpu.VMEM((2, 4, length, width), bf16),
            pltpu.VMEM((2, 4, length, width), bf16),
            pltpu.VMEM((2, 3, length, width), bf16),
            pltpu.VMEM((2, 3, length, width), bf16),
            pltpu.VMEM((length, width), bf16),
            pltpu.VMEM((length, count), f32),
        ]
        + [sem((4, 2)), sem((3, 2, line - 1)), sem((1 + max(1, down_weight.shape[1] // 128), line - 1)), sem((4,))]
        + [sem, sem((10,)), sem((2,)), sem((2, 2)), sem((2,)), sem((line + 1,))]
        + [sem((3,)), sem((4,)), sem((5,)), sem((2,))],
        compiler_params=pltpu.CompilerParams(
            collective_id=0, has_side_effects=True, vmem_limit_bytes=60 * 1024 * 1024
        ),
    )(*operands)
    layer_rows = pl.pallas_call(
        functools.partial(closing_kernel, n_fs, size),
        out_shape=jax.ShapeDtypeStruct((length, width), bf16),
        in_specs=[pl.BlockSpec(memory_space=pl.ANY)] * 3,
        out_specs=pl.BlockSpec(memory_space=pl.ANY),
        scratch_shapes=[pltpu.VMEM(*shape) for shape in late_shapes] + [sem((4,))],
        compiler_params=pltpu.CompilerParams(vmem_limit_bytes=60 * 1024 * 1024),
    )(*parts)
    return layer_rows.reshape(length, seq_count, width)


def solution(mesh):
    placed = (
        P("tp", ("rep", "fs"), None),
        P(),
        P("fs", "tp"),
        P("fs", "tp"),
        P(None, "tp"),
        P("tp"),
        P("tp", "fs"),
        P(),
        P("fs", "tp"),
        P("fs", "tp"),
        P("tp", "fs"),
    )
    return jax.shard_map(
        body, mesh=mesh, in_specs=placed, out_specs=P("tp", ("rep", "fs"), None), check_vma=False
    )
```

```python
import functools

import jax
import jax.numpy as jnp
from jax import lax
from jax.experimental import pallas as pl
from jax.experimental.pallas import tpu as pltpu
from jax.sharding import PartitionSpec as P

HEAD_DIM = 128
MESH = pl.DeviceIdType.MESH

norm_eps = 1e-06
group_eps = 1e-05
f32 = jnp.float32
bf16 = jnp.bfloat16


def rms_scale(matrix, scales):
    return matrix * lax.rsqrt(jnp.mean(matrix * matrix, axis=-1, keepdims=True) + norm_eps) * scales


MODULE, OUT, FFN, DOWN = range(4)


def nearest(place, line, t):
    left, right = place, line - 1 - place
    both = jnp.minimum(left, right)
    near = place - (t + 1) // 2 if t % 2 else place + t // 2
    far = jnp.where(right > left, place + (t - both), place - (t - both))
    return jnp.where(t <= 2 * both, near, far)


def final_columns(place, line, size):
    count = size if size % 128 == 0 else 2 * size
    block = (nearest(place, line, line - 1) * 2 * size + 2 * size - count) // count
    return block, count


class Moves:
    def __init__(self, n_rep, n_fs, sources, wholes, axes, sems):
        self.rep, self.fs, self.tp = lax.axis_index("rep"), lax.axis_index("fs"), lax.axis_index("tp")
        rep, fs, tp = self.rep, self.fs, self.tp
        self.n_fs, self.line = n_fs, n_fs // 2
        self.pair, self.place = fs % 2, fs // 2
        flip = fs + 1 - 2 * self.pair
        self.to_tp = (rep, fs, 1 - tp)
        self.peers = (None, (rep, flip, tp), (1 - rep, fs, tp), (1 - rep, flip, tp))
        self.ends = ((rep, (fs + 2) % n_fs, tp), (rep, (fs + n_fs - 2) % n_fs, tp))
        self.has = (self.place < self.line - 1, self.place > 0)
        self.quarter = rep * 2 + self.pair
        self.other = rep * 2 + 1 - self.pair
        self.sources, self.wholes, self.axes = sources, wholes, axes
        self.send, self.line_recv, self.down_recv, self.pair_recv = sems
        self.pieces = max(1, wholes[DOWN].shape[2] // 128)

    def greet(self):
        def signal(device):
            pl.semaphore_signal(pltpu.get_barrier_semaphore(), inc=1, device_id=device, device_id_type=MESH)

        for side in (0, 1):
            pl.when(self.has[side])(functools.partial(signal, self.ends[side]))
        for device in self.peers[1:] + (self.to_tp,):
            signal(device)

    def meet(self):
        inside = jnp.logical_and(*self.has)

        @pl.when(inside)
        def _():
            pl.semaphore_wait(pltpu.get_barrier_semaphore(), 6)

        @pl.when(jnp.logical_not(inside))
        def _():
            pl.semaphore_wait(pltpu.get_barrier_semaphore(), 5)

    def part(self, w, quarter):
        size = self.sources[w].shape[self.axes[w]] // 4
        at = pl.ds(pl.multiple_of(quarter * size, size), size)
        return (slice(None), at) if self.axes[w] == 1 else (at, slice(None))

    def slots(self, w, owner, count=1):
        if self.axes[w] == 0:
            return (owner,) if count == 1 else (pl.ds(owner, count),)
        size = self.sources[w].shape[0]
        return (pl.ds(pl.multiple_of(owner * size, size), count * size), slice(None))

    def copy(self, src, dst, device, send_sem, recv_sem):
        return pltpu.make_async_remote_copy(
            src_ref=src,
            dst_ref=dst,
            send_sem=send_sem,
            recv_sem=recv_sem,
            device_id=device,
            device_id_type=MESH,
        )

    def pair_copy(self, w):
        source, there = self.sources[w].at[self.part(w, self.other)], self.wholes[w].at[self.slots(w, self.fs)]
        return self.copy(source, there, self.peers[1], self.send.at[w, 0], self.pair_recv.at[w])

    def line_copy(self, w, p, owner, side, own=False):
        if w == DOWN:
            there = self.wholes[w].at[owner * 2 + min(p, 1)]
            if p:
                columns = there.shape[1] // self.pieces
                there = there.at[:, pl.ds((p - 1) * columns, columns)]
            recv_sem = self.down_recv.at[p, owner - side]
        else:
            parity = self.pair if p == 0 else 1 - self.pair
            there = self.wholes[w].at[self.slots(w, owner * 2 + parity)]
            recv_sem = self.line_recv.at[w, p, owner - side]
        here = self.sources[w].at[self.part(w, self.quarter)] if own and w != DOWN and p == 0 else there
        return self.copy(here, there, self.ends[side], self.send.at[w, side], recv_sem)

    def push_own_ffn(self, lead):
        rows = self.sources[FFN].shape[0]
        at = pl.ds(0, rows // 4) if lead else pl.ds(rows // 4, rows - rows // 4)
        there = self.wholes[FFN].at[self.slots(FFN, self.fs)].at[at, :]
        here = self.sources[FFN].at[self.part(FFN, self.quarter)].at[at, :]
        for side in (0, 1):


            @pl.when(self.has[side])
            def _():
                recv_sem = self.line_recv.at[FFN, 0, self.place - side]
                self.copy(here, there, self.ends[side], self.send.at[FFN, side], recv_sem).start()

    def push(self, w, p, s):
        if s == 1:
            if p == (0 if w == DOWN else 1):
                self.pair_copy(w).wait_recv()
            for side in (0, 1):


                @pl.when(self.has[side])
                def _():
                    self.line_copy(w, p, self.place, side, True).start()

            return
        for side in (0, 1):
            owner = self.place - (s - 1) if side == 0 else self.place + (s - 1)

            @pl.when((owner >= 0) if side == 0 else (owner < self.line))
            def _():
                copy = self.line_copy(w, p, owner, side)
                copy.wait_recv()
                pl.when(self.has[side])(copy.start)

    def arrived(self, w):
        for p in (0, 1):
            self.push(w, p, self.line)

    def sent(self):
        for place in range(self.line):

            @pl.when(self.place == place)
            def _():
                for w in range(4):
                    for side, count in ((0, place + 1), (1, self.line - place)):
                        count = (2 * count if count < self.line else 0) + 1 - side
                        if count:
                            shards = self.wholes[w].at[self.slots(w, 0, count)]
                            self.copy(shards, shards, self.peers[1], self.send.at[w, side], self.pair_recv.at[w]).wait_send()


class RowGather:
    def __init__(self, m, rows, send_sem, recv_sems):
        half = rows.shape[1] // 2
        low, high = pl.ds(0, half), pl.ds(half, half)
        _, pair, rep, _ = m.peers
        first, near_pair, near_rep, across = (2 * k + m.tp for k in range(4))
        moves = (
            (rows.at[first, low], rows.at[near_rep, low], rep),
            (rows.at[first, high], rows.at[near_pair, high], pair),
            (rows.at[first, high], rows.at[near_rep, high], rep),
            (rows.at[first, low], rows.at[near_pair, low], pair),
            (rows.at[near_rep, low], rows.at[across, low], pair),
            (rows.at[near_pair, high], rows.at[across, high], rep),
            (rows.at[first], rows.at[first], m.to_tp),
            (rows.at[near_rep], rows.at[near_rep], m.to_tp),
            (rows.at[near_pair], rows.at[near_pair], m.to_tp),
            (rows.at[across], rows.at[across], m.to_tp),
        )
        self.copies = [m.copy(*move, send_sem, recv_sems.at[4 if i == 5 else i]) for i, move in enumerate(moves)]
        self.diagonal = m.copy(rows.at[across], rows.at[across], pair, send_sem, recv_sems.at[4])
        seven = rows.at[pl.ds(0, 7)]
        self.all_sent = m.copy(seven, seven, pair, send_sem, recv_sems.at[0])

    def start(self):
        for i in (0, 1, 2, 3, 6):
            self.copies[i].start()

    def forward(self):
        for i in (0, 1):
            self.copies[i].wait_recv()
            self.copies[i + 4].start()

    def finish(self):
        for i in (2, 3):
            self.copies[i].wait_recv()
            self.copies[i + 5].start()
        self.diagonal.wait_recv()
        self.copies[9].start()

    def ready(self, k):
        for i in ((6,), (8,), (7,), (9,))[k]:
            self.copies[i].wait_recv()

    def sent(self):
        self.all_sent.wait_send()


def layer_kernel(
    n_rep, n_fs, tokens_in, mix_gain_in, value, gate, taps_in, head_gain_in, out, ffn_gain_in, ffn_gate, ffn_up,
    down, early, partial, late,
    *scratch,
):
    staged, wholes, scratch = scratch[:4], scratch[4:8], scratch[8:]
    module_q, out_q, ffn_q, down_q = wholes
    tokens, mix_gain, taps, head_gain, ffn_gain = scratch[:5]
    rows_a, rows, padded, activated, hidden, middle, total, tp_out, tp_in, x_out, x_in, finished, last_partial = scratch[5:18]
    weight_sems, scratch = scratch[18:22], scratch[22:]
    row_send, row_recv, tp_send, tp_recv, x_send, x_first, x_last, stage_sem, small_sem, end_sem = scratch
    channels, units = out_q.shape[1], down_q.shape[1]
    m = Moves(n_rep, n_fs, staged, wholes, (1, 0, 1, 0), weight_sems)
    length, width = tokens.shape
    kernel = taps.shape[0]
    pad = (padded.shape[1] - 2 * length) // 2
    tile = 512
    high = 32
    near_at = pl.ds(pl.multiple_of(m.tp * length, length), length)
    far_at = pl.ds(pl.multiple_of((1 - m.tp) * length, length), length)

    def stage(w, shards):
        if len(shards) == 1:
            pltpu.make_async_copy(shards[0], staged[w], stage_sem.at[w]).start()
            return
        size = shards[0].shape[1] // 4
        for i, shard in enumerate(shards):
            for q in range(4):
                there = staged[w].at[:, pl.ds((2 * q + i) * size, size)]
                pltpu.make_async_copy(shard.at[:, pl.ds(q * size, size)], there, stage_sem.at[w]).start()

    def stage_wait(w):
        pltpu.make_async_copy(staged[w], staged[w], stage_sem.at[w]).wait()

    def place(w, wait):
        there = wholes[w].at[m.slots(w, m.fs)]
        copy = pltpu.make_async_copy(staged[w].at[m.part(w, m.quarter)], there, stage_sem.at[w])
        copy.wait() if wait else copy.start()

    smalls = ((tokens_in, tokens), (mix_gain_in, mix_gain), (taps_in, taps))
    smalls += ((head_gain_in, head_gain), (ffn_gain_in, ffn_gain))
    small = [pltpu.make_async_copy(s, d, small_sem.at[i]) for i, (s, d) in enumerate(smalls)]
    m.greet()
    stage(MODULE, (value, gate))
    stage(OUT, (out,))
    small[0].start()
    small[1].start()
    stage(FFN, (ffn_gate, ffn_up))
    stage(DOWN, (down,))
    for copy in small[2:]:
        copy.start()
    stage_wait(MODULE)
    m.meet()
    m.pair_copy(MODULE).start()
    m.push(MODULE, 0, 1)
    stage_wait(OUT)
    m.pair_copy(OUT).start()
    m.push(OUT, 0, 1)
    stage_wait(FFN)
    m.push_own_ffn(True)

    def module_norm(i, _):
        at = pl.ds(pl.multiple_of(i * high, high), high)
        rows_a[m.tp, at, :] = rms_scale(tokens[at, :].astype(f32), mix_gain[...]).astype(bf16)
        return _

    small[0].wait()
    small[1].wait()
    lax.fori_loop(0, length // high, module_norm, 0)
    gather = RowGather(m, rows_a, row_send, row_recv)
    gather.start()
    m.push(MODULE, 1, 1)
    stage_wait(DOWN)
    for w in (MODULE, OUT, FFN, DOWN):
        place(w, False)
    zeros = jnp.zeros((4, pad, channels), f32)
    padded[:, pl.ds(0, pad), :] = zeros
    padded[:, pl.ds(pad + 2 * length, pad), :] = zeros
    for s in range(2, m.line):
        m.push(MODULE, 0, s)
        if s > 2:
            m.push(OUT, 0, s - 1)
        m.push(OUT, 1, s - 1)
        m.push(MODULE, 1, s)
        if s == 2:
            gather.forward()
            m.pair_copy(FFN).start()
    for p in (0, 1):
        m.push(OUT, p, m.line - 1)
    m.push_own_ffn(False)
    gather.finish()
    for w in (MODULE, OUT, FFN, DOWN):
        place(w, True)
    for copy in small[2:]:
        copy.wait()
    m.arrived(MODULE)

    def gated(k):
        block = rows_a[pl.ds(2 * k, 2)].reshape(2 * length, width)
        both = jnp.dot(block, module_q[...], preferred_element_type=f32)
        glu = (both[:, :channels] * jax.nn.sigmoid(both[:, channels:])).astype(bf16)
        padded[k, pl.ds(pad, 2 * length), :] = glu.astype(f32)

    channels_at = pl.ds(pl.multiple_of(m.quarter * channels, channels), channels)
    conv_rows = 64

    def convolve(k, _):
        for first in range(0, 2 * length, conv_rows):
            conved = jnp.zeros((conv_rows, channels), f32)
            for t in range(kernel):
                shifted = padded[k, pl.ds(first + t + pad - kernel // 2, conv_rows), :]
                conved = conved + shifted * taps[pl.ds(t, 1), channels_at]
            gains = head_gain[:, channels_at]
            for g in range(0, channels, HEAD_DIM):
                grouped = conved[:, g : g + HEAD_DIM]
                head_mean = jnp.mean(grouped, axis=-1, keepdims=True)
                head_var = jnp.mean(jnp.square(grouped - head_mean), axis=-1, keepdims=True)
                scaled = (grouped - head_mean) * lax.rsqrt(head_var + group_eps) * gains[:, g : g + HEAD_DIM]
                activated[k, pl.ds(first, conv_rows), pl.ds(g, HEAD_DIM)] = jax.nn.silu(scaled).astype(bf16)
        return _

    for k in range(4):
        gather.ready(k)
        gated(k)
    m.push(FFN, 1, 1)
    lax.fori_loop(0, 4, convolve, 0)
    m.arrived(OUT)

    def columns(weight, c):
        slots = tile // weight.shape[2]
        return jnp.concatenate([weight[c * slots + i] for i in range(slots)], axis=1)

    def tile_loop(step):
        def run(c, _):
            step(columns(out_q, c), pl.ds(pl.multiple_of(c * tile, tile), tile))
            return _

        lax.fori_loop(0, width // tile, run, 0)

    size = down_q.shape[2]
    last_t = m.line - 1
    phases = [None] + [(t, 0, 2 * size) for t in range(last_t)]
    if size % 128 == 0:
        phases += [(last_t, 0, size)] + [(last_t, size + c, 128) for c in range(0, size, 128)]
    else:
        phases += [(last_t, 0, 2 * size)]
    final = len(phases) - 1
    direct = [i for i in range(1, final + 1) if phases[i][0] == last_t and (phases[i][1] or i == final)]

    def phase_base(phase):
        return nearest(m.place, m.line, phases[phase][0]) * 2

    def phase_columns(phase):
        if phase == 0:
            return slice(None)
        _, first, count = phases[phase]
        return pl.ds(pl.multiple_of(phase_base(phase) * size + first, count), count)

    def phase_weight(phase):
        _, first, count = phases[phase]
        base = phase_base(phase)
        if count == 2 * size:
            return jnp.concatenate([down_q[base], down_q[base + 1]], axis=1)
        return down_q[base + first // size, :, pl.ds(first % size, count)]

    def tp_copy(phase, k, count=1):
        b, at = min(phase, 1), (pl.ds(k, count), slice(None), phase_columns(phase))
        recv_sem = tp_recv.at[phase % 2, 0 if k == 3 else 1]
        return m.copy(tp_out.at[(b, *at)], tp_in.at[(b, *at)], m.to_tp, tp_send.at[b], recv_sem)

    def x_copy(phase, k, low):
        b, columns_at = min(phase, 1), phase_columns(phase)
        at = pl.ds(0, length // 2) if low else pl.ds(length // 2, length // 2)
        to_rep = k == 2 or (k == 3 and low)
        there = (b, k - 1, at, columns_at)
        recv_sem = x_first.at[phase] if k == 3 else x_last.at[b]
        return m.copy(x_out.at[there], x_in.at[there], m.peers[2 if to_rep else 1], x_send.at[b], recv_sem)

    def direct_copy(phase, k):
        source = x_out.at[1, k - 1, :, phase_columns(phase)]
        first, count = phases[phase][1] - phases[direct[0]][1], phases[phase][2]
        return m.copy(source, late.at[k - 1, :, pl.ds(first, count)], m.peers[k], x_send.at[1], x_last.at[2])

    def received(ref, sem):
        m.copy(ref, ref, m.peers[1], x_send.at[0], sem).wait_recv()

    def far_sums(k):
        def step(weight, at):
            product = jnp.dot(activated[k, far_at, :], weight, preferred_element_type=f32)
            tp_out[0, k, :, at] = product.astype(bf16)

        tile_loop(step)
        tp_copy(0, k).start()

    def near_sums(k):
        def step(weight, at):
            part = jnp.dot(activated[k, near_at, :], weight, preferred_element_type=f32)
            part = part + tp_in[0, k, :, at].astype(f32)
            if k == 0:
                total[0, :, at] = part
            else:
                x_out[0, k - 1, :, at] = part.astype(bf16)

        tile_loop(step)
        if k == 3:
            x_copy(0, 3, 1).start()
            x_copy(0, 3, 0).start()
        elif k:
            x_copy(0, k, k - 1).start()

    def ffn_far_sums(phase):
        _, _, count = phases[phase]
        product = jnp.dot(
            hidden[1 - m.tp].reshape(4 * length, units), phase_weight(phase), preferred_element_type=f32
        )
        tp_out[1, :, :, phase_columns(phase)] = product.astype(bf16).reshape(4, length, count)
        tp_copy(phase, 3).start()
        tp_copy(phase, 0, 3).start()

    def ffn_near_sums(phase):
        at = phase_columns(phase)
        parts = jnp.dot(hidden[m.tp].reshape(4 * length, units), phase_weight(phase), preferred_element_type=f32)
        tp_copy(phase, 3).wait_recv()
        for k in (3, 2, 1, 0):
            if k == 2:
                tp_copy(phase, 0, 3).wait_recv()
            part = parts[k * length : (k + 1) * length] + tp_in[1, k, :, at].astype(f32)
            if k == 0:
                total[1, :, at] = part
                continue
            x_out[1, k - 1, :, at] = part.astype(bf16)
            if phase in direct:
                direct_copy(phase, k).start()
            elif k == 3:
                x_copy(phase, 3, 1).start()
                x_copy(phase, 3, 0).start()
            else:
                x_copy(phase, k, k - 1).start()

    def forward_sums(phase):
        b, columns_at = min(phase, 1), phase_columns(phase)
        received(x_in.at[b, 2, :, columns_at], x_first.at[phase])
        for k, low in ((1, 1), (2, 0)):
            first = 0 if low else length // 2

            def add(i, _):
                at = pl.ds(pl.multiple_of(first + i * high, high), high)
                part = x_out[b, k - 1, at, columns_at].astype(f32)
                part = part + x_in[b, 2, at, columns_at].astype(f32)
                x_out[b, k - 1, at, columns_at] = part.astype(bf16)
                return _

            lax.fori_loop(0, length // (2 * high), add, 0)
            x_copy(phase, k, low).start()

    def sums_sent(b):
        m.copy(tp_out.at[b], tp_out.at[b], m.to_tp, tp_send.at[b], x_last.at[b]).wait_send()
        m.copy(x_out.at[b], x_out.at[b], m.peers[1], x_send.at[b], x_last.at[b]).wait_send()

    def all_sums(b, at):
        part = total[b, at, :]
        for k in (1, 2):
            part = part + x_in[b, k - 1, at, :].astype(f32)
        return part

    far_sums(3)
    far_sums(2)
    tp_copy(0, 3).wait_recv()
    near_sums(3)
    far_sums(1)
    far_sums(0)
    tp_copy(0, 0, 3).wait_recv()
    for k in (2, 1, 0):
        near_sums(k)
    m.push(FFN, 0, 2)
    forward_sums(0)
    m.push(FFN, 1, 2)
    m.pair_copy(DOWN).start()
    gather.sent()
    received(x_in.at[0, pl.ds(0, 2)], x_last.at[0])

    def norm_rows(i, _):
        at = pl.ds(pl.multiple_of(i * high, high), high)
        mid = (tokens[at, :].astype(f32) + all_sums(0, at)).astype(bf16)
        middle[at, :] = mid
        rows[m.tp, at, :] = rms_scale(mid.astype(f32), ffn_gain[...]).astype(bf16)
        return _

    lax.fori_loop(0, length // high, norm_rows, 0)
    gather = RowGather(m, rows, row_send, row_recv)
    gather.start()
    for s in range(3, m.line):
        for p in (0, 1):
            m.push(FFN, p, s)
        if s == 3:
            gather.forward()
    if m.line < 4:
        gather.forward()
    for p in range(1 + m.pieces):
        m.push(DOWN, p, 1)
    gather.finish()
    for k in range(4):
        gather.ready(k)
    m.arrived(FFN)

    def feed(i, _):
        at = pl.ds(2 * i, 2)
        block = rows[at].reshape(2 * length, width)
        both = jnp.dot(block, ffn_q[...], preferred_element_type=f32)
        block = (jax.nn.silu(both[:, :units]) * both[:, units:]).astype(bf16)
        hidden[0, i] = block[:length]
        hidden[1, i] = block[length:]
        return _

    lax.fori_loop(0, 4, feed, 0)
    m.push(DOWN, 0, 2)
    for phase in range(1, final + 1):
        t, first, count = phases[phase]
        for p in range(1 + m.pieces):
            begin = p if p == 0 else size + (p - 1) * size // m.pieces
            if t and (t, p) != (1, 0) and (t < last_t or first <= begin < first + count):
                m.push(DOWN, p, t + 1)
        ffn_far_sums(phase)
        if phase == final:
            forward_sums(direct[0] - 1)
        ffn_near_sums(phase)
        if 1 < phase < direct[0]:
            forward_sums(phase - 1)
    final_block, count = final_columns(m.place, m.line, size)
    final_at = pl.ds(pl.multiple_of(final_block * count, count), count)
    last_partial[...] = middle[:, final_at].astype(f32) + total[1, :, final_at]
    keep = pltpu.make_async_copy(last_partial, partial, end_sem.at[0])
    keep.start()
    blocks = width // count
    before_final = pl.ds(0, width - count)
    received(x_in.at[1, pl.ds(0, 2), :, before_final], x_last.at[1])

    def finish(j, _):
        block = (final_block + j) % blocks
        at = pl.ds(pl.multiple_of(block * count, count), count)
        done = middle[:, at].astype(f32) + total[1, :, at]
        for k in range(2):
            done = done + x_in[1, k, :, at].astype(f32)
        finished[:, at] = done.astype(bf16)
        pltpu.make_async_copy(finished.at[:, at], early.at[:, at], end_sem.at[1]).start()
        return _

    lax.fori_loop(1, blocks, finish, 0)
    gather.sent()
    sums_sent(0)
    m.sent()
    others = finished.at[:, before_final]
    pltpu.make_async_copy(others, others, end_sem.at[1]).wait()
    keep.wait()
    sums_sent(1)
    received(late, x_last.at[2])


def closing_kernel(n_fs, size, early, partial, late, result, rows, last, parts, sems):
    block, count = final_columns(lax.axis_index("fs") // 2, n_fs // 2, size)
    copies = [
        pltpu.make_async_copy(source, there, sems.at[i])
        for i, (source, there) in enumerate(((early, rows), (partial, last), (late, parts)))
    ]
    for copy in copies:
        copy.start()
    for copy in copies:
        copy.wait()
    done = last[...]
    for k in range(3):
        done = done + parts[k].astype(f32)
    rows[:, pl.ds(pl.multiple_of(block * count, count), count)] = done.astype(bf16)
    leave = pltpu.make_async_copy(rows, result, sems.at[3])
    leave.start()
    leave.wait()


def body(
    tokens,
    mix_gain,
    value_weight,
    gate_weight,
    conv_taps,
    head_gain,
    out_weight,
    ffn_gain,
    ffn_gate_weight,
    ffn_up_weight,
    down_weight,
):
    n_rep, n_fs, n_tp = lax.axis_size("rep"), lax.axis_size("fs"), lax.axis_size("tp")
    length, seq_count, width = tokens.shape
    assert n_rep == 2 and n_tp == 2 and n_fs % 2 == 0 and n_fs > 4 and seq_count == 1
    line = n_fs // 2
    kernel = conv_taps.shape[0]
    channels, units = out_weight.shape[0] // 4, down_weight.shape[0] // 4
    pad = -(-(kernel // 2) // 8) * 8
    sem = pltpu.SemaphoreType.DMA
    operands = (
        tokens.reshape(length, width),
        mix_gain.reshape(1, width),
        value_weight,
        gate_weight,
        conv_taps,
        head_gain.reshape(1, -1),
        out_weight,
        ffn_gain.reshape(1, width),
        ffn_gate_weight,
        ffn_up_weight,
        down_weight,
    )
    size = down_weight.shape[1]
    count = size if size % 128 == 0 else 2 * size
    late_shapes = (((length, width), bf16), ((length, count), f32), ((3, length, count), bf16))
    parts = pl.pallas_call(
        functools.partial(layer_kernel, n_rep, n_fs),
        out_shape=[jax.ShapeDtypeStruct(*shape) for shape in late_shapes],
        in_specs=[pl.BlockSpec(memory_space=pl.ANY)] * len(operands),
        out_specs=[pl.BlockSpec(memory_space=pl.ANY)] * 3,
        scratch_shapes=[
            pltpu.VMEM((value_weight.shape[0], 8 * channels), bf16),
            pltpu.VMEM(out_weight.shape, bf16),
            pltpu.VMEM((ffn_gate_weight.shape[0], 8 * units), bf16),
            pltpu.VMEM(down_weight.shape, bf16),
            pltpu.VMEM((width, 2 * channels), bf16),
            pltpu.VMEM((n_fs, channels, out_weight.shape[1]), bf16),
            pltpu.VMEM((width, 2 * units), bf16),
            pltpu.VMEM((n_fs, units, down_weight.shape[1]), bf16),
            pltpu.VMEM((length, width), bf16),
            pltpu.VMEM((1, width), f32),
            pltpu.VMEM(conv_taps.shape, f32),
            pltpu.VMEM((1, head_gain.shape[0]), f32),
            pltpu.VMEM((1, width), f32),
            pltpu.VMEM((8, length, width), bf16),
            pltpu.VMEM((8, length, width), bf16),
            pltpu.VMEM((4, 2 * length + 2 * pad, channels), f32),
            pltpu.VMEM((4, 2 * length, channels), bf16),
            pltpu.VMEM((2, 4, length, units), bf16),
            pltpu.VMEM((length, width), bf16),
            pltpu.VMEM((2, length, width), f32),
            pltpu.VMEM((2, 4, length, width), bf16),
            pltpu.VMEM((2, 4, length, width), bf16),
            pltpu.VMEM((2, 3, length, width), bf16),
            pltpu.VMEM((2, 3, length, width), bf16),
            pltpu.VMEM((length, width), bf16),
            pltpu.VMEM((length, count), f32),
        ]
        + [sem((4, 2)), sem((3, 2, line - 1)), sem((1 + max(1, down_weight.shape[1] // 128), line - 1)), sem((4,))]
        + [sem, sem((10,)), sem((2,)), sem((2, 2)), sem((2,)), sem((line + 1,))]
        + [sem((3,)), sem((4,)), sem((5,)), sem((2,))],
        compiler_params=pltpu.CompilerParams(
            collective_id=0, has_side_effects=True, vmem_limit_bytes=60 * 1024 * 1024
        ),
    )(*operands)
    layer_rows = pl.pallas_call(
        functools.partial(closing_kernel, n_fs, size),
        out_shape=jax.ShapeDtypeStruct((length, width), bf16),
        in_specs=[pl.BlockSpec(memory_space=pl.ANY)] * 3,
        out_specs=pl.BlockSpec(memory_space=pl.ANY),
        scratch_shapes=[pltpu.VMEM(*shape) for shape in late_shapes] + [sem((4,))],
        compiler_params=pltpu.CompilerParams(vmem_limit_bytes=60 * 1024 * 1024),
    )(*parts)
    return layer_rows.reshape(length, seq_count, width)


def solution(mesh):
    placed = (
        P("tp", ("rep", "fs"), None),
        P(),
        P("fs", "tp"),
        P("fs", "tp"),
        P(None, "tp"),
        P("tp"),
        P("tp", "fs"),
        P(),
        P("fs", "tp"),
        P("fs", "tp"),
        P("tp", "fs"),
    )
    return jax.shard_map(
        body, mesh=mesh, in_specs=placed, out_specs=P("tp", ("rep", "fs"), None), check_vma=False
    )
```
